128 devices in a mesh: sp: 16 (over z, y), tp: 4 (over x), dp: 2 (over core).
Axes of the slice: x: 4, y: 4, z: 4, core: 2. Of those that a mesh axis runs over, the one named last changes fastest.
Arguments:
- latent: bfloat16 [2, 12288, 2048], P('dp', ('sp', 'tp')), may hold values from -3 to 3
- cond: bfloat16 [2, 2048], P('dp', 'sp'), may hold values from -6 to 6
- cond_ctx: bfloat16 [2048], P('sp'), may hold values from -6 to 6
- context: bfloat16 [2, 512, 2048], P('dp', 'sp'), may hold values from -6 to 6
- norm_gain: bfloat16 [2048], replicated, may hold values from 0.099609375 to 1.8984375
- mod_shift: bfloat16 [2048, 2048], P('sp', 'tp'), may hold values from -0.125 to 0.125
- mod_scale: bfloat16 [2048, 2048], P('sp', 'tp'), may hold values from -0.125 to 0.125
- mod_gate: bfloat16 [2048, 2048], P('sp', 'tp'), may hold values from -0.125 to 0.125
- w_query: bfloat16 [2048, 1024], P(None, 'tp'), may hold values from -0.125 to 0.125
- w_key: bfloat16 [2048, 256], P(None, 'tp'), may hold values from -0.125 to 0.125
- w_value: bfloat16 [2048, 256], P(None, 'tp'), may hold values from -0.125 to 0.125
- q_gain: bfloat16 [64], replicated, may hold values from 1 to 5.5
- k_gain: bfloat16 [64], replicated, may hold values from 1 to 5.5
- ctx_lift: float32 [16], P('tp'), may hold values from 1 to 3
- w_out: bfloat16 [1024, 2048], replicated, may hold values from -1.5 to 1.5
Outputs:
- mixed: bfloat16 [2, 12288, 2048], P('dp', ('sp', 'tp'))
The draws below stay inside these ranges and needn't reach their ends.
All inputs are finite; a program needn't handle non-finite values.
Results may differ from the reference program's by a relative error of at most 0.009.
The reference program's roundings to bfloat16 on the way count: a program that leaves them out, or rounds other values in their place, can miss the bound.
Values may be sent and summed in bfloat16 or wider, within the bound.
A program may use at most 64 MiB of HBM per device.

```python
import jax
import jax.numpy as jnp
from jax import lax

D = 2048
HEADS = 16
KV_HEADS = 4
HD = 64
GRID_W = 128
TOK_DEV = 768
CTX = 512
SAMPLES = 2
LAT = 12288
QW = 1024
KVW = 256
N_SP = 16


def draw_gain(key, salt):
    base = jax.random.uniform(jax.random.fold_in(key, salt), (HD,), jnp.float32, 1.0, 1.8)
    return base.astype(jnp.bfloat16)


def draw_q_gain(key, part):
    return draw_gain(key, 1)


def draw_k_gain(key, part):
    return draw_gain(key, 2)


def level_of(rng, shape, shards, low, top_value):
    def one(dim, blocks):
        draws = jax.random.uniform(jax.random.fold_in(jax.random.fold_in(rng, 6), dim), (blocks,), jnp.float32, low / len(shards), top_value / len(shards))
        return jnp.repeat(jnp.exp(draws), shape[dim] // blocks).reshape((-1,) + (1,) * (len(shape) - dim - 1))

    level = one(*shards[0])
    for cut in shards[1:]:
        level = level * one(*cut)
    return level


def bell_draw(key, dims, spread, reach, shards=(), held_as=jnp.bfloat16):
    entries = spread * jax.random.normal(key, dims, jnp.float32)
    if shards:
        entries = entries * level_of(key, dims, shards, -0.22, 0.18)
    return jnp.clip(entries, -reach, reach).astype(held_as)


def setup_inputs(seed: int = 0) -> dict:
    arg_keys = jax.random.split(jax.random.key(seed), 16)
    return {
        "latent": bell_draw(arg_keys[0], (SAMPLES, LAT, D), 0.5, 3.0, ((0, 2), (1, 64))),
        "cond": bell_draw(arg_keys[1], (SAMPLES, D), 1.0, 6.0, ((0, 2), (1, 16))),
        "cond_ctx": bell_draw(arg_keys[2], (D,), 1.0, 6.0, ((0, 16),)),
        "context": bell_draw(arg_keys[3], (SAMPLES, CTX, D), 1.0, 6.0, ((0, 2), (1, 16))),
        "norm_gain": jnp.clip(1.0 + 0.18 * jax.random.normal(arg_keys[4], (D,), jnp.float32), 0.099609375, 1.8984375).astype(jnp.bfloat16),
        "mod_shift": bell_draw(arg_keys[5], (D, D), D ** -0.5, 0.125, ((0, 16), (1, 4))),
        "mod_scale": bell_draw(arg_keys[6], (D, D), D ** -0.5, 0.125, ((0, 16), (1, 4))),
        "mod_gate": bell_draw(arg_keys[7], (D, D), D ** -0.5, 0.125, ((0, 16), (1, 4))),
        "w_query": bell_draw(arg_keys[8], (D, QW), D ** -0.5, 0.125, ((1, 4),)),
        "w_key": bell_draw(arg_keys[9], (D, KVW), D ** -0.5, 0.125, ((1, 4),)),
        "w_value": bell_draw(arg_keys[10], (D, KVW), D ** -0.5, 0.125, ((1, 4),)),
        "q_gain": draw_q_gain(jax.random.fold_in(arg_keys[15], 71), 0),
        "k_gain": draw_k_gain(jax.random.fold_in(arg_keys[15], 71), 0),
        "ctx_lift": jnp.clip(1.0 + 2.0 * jax.random.uniform(arg_keys[13], (HEADS,), jnp.float32) ** level_of(arg_keys[13], (HEADS,), ((0, 4),), -0.2, 0.2), 1.0, 3.0),
        "w_out": bell_draw(arg_keys[14], (QW, D), (QW // 64) ** -0.5, 1.5),
    }


EPS = 1e-06
THETA = 10000.0

def modulate(row_block, gain_vec, shift_rows, scale_rows):
    values = row_block.astype(jnp.float32)
    normed = values * lax.rsqrt(lax.optimization_barrier(jnp.mean(values * values, axis=-1, keepdims=True)) + EPS) * gain_vec.astype(jnp.float32)
    return (normed * (1.0 + scale_rows) + shift_rows).astype(jnp.bfloat16)

def head_norm(raw_proj, gain_vec):
    samples, tokens, width = raw_proj.shape
    pieces = raw_proj.reshape(samples, tokens, width // HD, HD)
    normed = pieces * lax.rsqrt(lax.optimization_barrier(jnp.mean(pieces * pieces, axis=-1, keepdims=True)) + EPS) * gain_vec.astype(jnp.float32)
    return normed.transpose(0, 2, 1, 3)

def rotate(vector, positions):
    pairs_count = vector.shape[-1] // 4
    grid_row = (positions // GRID_W).astype(jnp.float32)
    grid_col = (positions % GRID_W).astype(jnp.float32)
    inverse = THETA ** (-jnp.arange(pairs_count, dtype=jnp.float32) / pairs_count)
    angles = jnp.concatenate([grid_row[:, None] * inverse, grid_col[:, None] * inverse], axis=-1)
    cosine = jnp.cos(angles)
    sine_val = jnp.sin(angles)
    first_half = vector[..., 0::2]
    second_half = vector[..., 1::2]
    turned = jnp.stack([first_half * cosine - second_half * sine_val, first_half * sine_val + second_half * cosine], axis=-1)
    return turned.reshape(vector.shape)

def attend_head(operands):
    query_head, key_head, value_head, ctx_key_head, ctx_value_head, lift_row = operands
    group_size = query_head.shape[0]
    factor = HD ** (-0.5)
    query_blocks = jnp.moveaxis(query_head.reshape(group_size, N_SP, TOK_DEV, HD), 1, 0)

    def one_block(query_block):
        query_wide = query_block.astype(jnp.float32)
        scores = jnp.einsum('gbd,td->gbt', query_wide, key_head.astype(jnp.float32)) * factor
        ctx_scores = jnp.einsum('gbd,td->gbt', query_wide, ctx_key_head.astype(jnp.float32)) * factor + lift_row[:, None, None]
        peak = jnp.maximum(lax.optimization_barrier(jnp.max(scores, axis=-1)), lax.optimization_barrier(jnp.max(ctx_scores, axis=-1)))
        weights = jnp.exp(scores - peak[..., None])
        ctx_weights = jnp.exp(ctx_scores - peak[..., None])
        total = lax.optimization_barrier(jnp.sum(weights, axis=-1)) + lax.optimization_barrier(jnp.sum(ctx_weights, axis=-1))
        weights_low = lax.optimization_barrier(weights.astype(jnp.bfloat16)).astype(jnp.float32)
        ctx_low = lax.optimization_barrier(ctx_weights.astype(jnp.bfloat16)).astype(jnp.float32)
        summed = jnp.einsum('gbt,td->gbd', weights_low, value_head.astype(jnp.float32))
        summed = summed + jnp.einsum('gbt,td->gbd', ctx_low, ctx_value_head.astype(jnp.float32))
        return (summed / total[..., None]).astype(jnp.bfloat16)
    outputs = lax.map(one_block, query_blocks)
    return jnp.moveaxis(outputs, 0, 1).reshape(group_size, N_SP * TOK_DEV, HD)

def reference(latent, cond, cond_ctx, context, norm_gain, mod_shift, mod_scale, mod_gate, w_query, w_key, w_value, q_gain, k_gain, ctx_lift, w_out):
    samples = latent.shape[0]
    tokens = latent.shape[1]
    group_size = HEADS // KV_HEADS
    active = jax.nn.silu(jnp.concatenate([cond, cond_ctx[None, :]], axis=0).astype(jnp.float32)).astype(jnp.bfloat16)
    shift_rows = jnp.dot(active, mod_shift, preferred_element_type=jnp.float32)
    scale_rows = jnp.dot(active, mod_scale, preferred_element_type=jnp.float32)
    gate_rows = jnp.dot(active, mod_gate, preferred_element_type=jnp.float32)
    modulated = modulate(latent, norm_gain, shift_rows[:samples, None, :], scale_rows[:samples, None, :])
    ctx_mod = modulate(context, norm_gain, shift_rows[samples], scale_rows[samples])
    flat = modulated.reshape(-1, D)
    ctx_flat = ctx_mod.reshape(-1, D)
    qraw = jnp.dot(flat, w_query, preferred_element_type=jnp.float32).reshape(samples, tokens, QW)
    kraw = jnp.dot(flat, w_key, preferred_element_type=jnp.float32).reshape(samples, tokens, KVW)
    value_rows = jnp.dot(flat, w_value, preferred_element_type=jnp.float32).astype(jnp.bfloat16)
    kcraw = jnp.dot(ctx_flat, w_key, preferred_element_type=jnp.float32).reshape(samples, CTX, KVW)
    ctx_value_rows = jnp.dot(ctx_flat, w_value, preferred_element_type=jnp.float32).astype(jnp.bfloat16)
    positions = jnp.arange(tokens, dtype=jnp.int32)
    queries = rotate(head_norm(qraw, q_gain), positions).astype(jnp.bfloat16)
    queries = queries.reshape(samples, KV_HEADS, group_size, tokens, HD)
    key_rows = rotate(head_norm(kraw, k_gain), positions).astype(jnp.bfloat16)
    value_heads = value_rows.reshape(samples, tokens, KV_HEADS, HD).transpose(0, 2, 1, 3)
    ctx_keys = head_norm(kcraw, k_gain).astype(jnp.bfloat16)
    ctx_values = ctx_value_rows.reshape(samples, CTX, KV_HEADS, HD).transpose(0, 2, 1, 3)
    lift_table = ctx_lift.astype(jnp.float32).reshape(KV_HEADS, group_size)
    results = []
    for sample_idx in range(samples):
        attended = lax.map(attend_head, (queries[sample_idx], key_rows[sample_idx], value_heads[sample_idx], ctx_keys[sample_idx], ctx_values[sample_idx], lift_table))
        results.append(attended.transpose(2, 0, 1, 3).reshape(tokens, QW))
    head_rows = jnp.stack(results, axis=0)
    projected = jnp.dot(head_rows.reshape(-1, QW), w_out, preferred_element_type=jnp.float32).reshape(samples, tokens, D)
    return (latent.astype(jnp.float32) + gate_rows[:samples, None, :] * projected).astype(jnp.bfloat16)
```

```python
import functools

import jax
import jax.numpy as jnp
import numpy as np
from jax import lax
from jax.experimental import pallas as pl
from jax.experimental.pallas import tpu as pltpu
from jax.sharding import PartitionSpec as P

HD = 64
GRID_W = 128
EPS = 1e-06
THETA = 10000.0
MESH = pl.DeviceIdType.MESH
LOG2E = 1.4426950408889634
QB = 256
KB = 256


def rope_tables(grid_rows):
    n = HD // 4
    inverse = (np.float32(THETA) ** (-np.arange(n, dtype=np.float32) / np.float32(n))).astype(np.float32)

    def table(count, low):
        angles = (np.arange(count, dtype=np.float32)[:, None] * inverse).astype(np.float32)
        zero = np.zeros((count, 2 * n), np.float32)
        sign = np.tile(np.array([-1.0, 1.0], np.float32), n)
        c = np.repeat(np.cos(angles.astype(np.float64)), 2, axis=1).astype(np.float32)
        s = np.repeat(np.sin(angles.astype(np.float64)), 2, axis=1).astype(np.float32) * sign
        parts = ([c, zero], [s, zero]) if low else ([zero, c], [zero, s])
        return [np.tile(np.concatenate(p, axis=1), (1, 2)) for p in parts]

    return np.stack(table(grid_rows, True)), np.stack(table(GRID_W, False))


def kernel(
    n_sp, n_tp, group,
    latent, cond, cond_ctx, norm_gain, q_gain, k_gain, lift, row_tab, col_tab,
    context_h, mshift_h, mscale_h, mgate_h, wq_h, wk_h, wv_h, wout_h,
    out,
    context, mods_w, wq, wk, wv, wkv, wout,
    raw, part, part_in, mods_all, ab, rope, q_tok, q_t, kv_all, kv_ctx, v_t, s_a, s_b, acc, m_st, o_tok, o_all,
    local_sem, lat_send, lat_recv, pa_send, pa_recv, pb_send, pb_recv, kv_send, kv_recv, o_ssem, o_rsem,
):
    rows = latent.shape[0]
    half = rows // 2
    width = latent.shape[1]
    chunk = width // n_tp
    tokens = rows * n_tp
    ctx_rows = context.shape[0]
    sp = lax.axis_index("sp")
    tp = lax.axis_index("tp")
    tx, ty = tp % 2, tp // 2
    peers = (ty * 2 + (1 - tx), (1 - ty) * 2 + tx, (1 - ty) * 2 + (1 - tx))
    sp_order = sorted(range(1, n_sp), key=lambda d: min(d, n_sp - d))

    local = [
        pltpu.make_async_copy(src, dst, local_sem.at[i])
        for i, (src, dst) in enumerate(
            (
                (mshift_h, mods_w.at[0]),
                (mscale_h, mods_w.at[1]),
                (mgate_h, mods_w.at[2]),
                (context_h, context),
                (wk_h, wk),
                (wv_h, wv),
                (wq_h, wq),
                (wout_h, wout),
            )
        )
    ]
    for copy in local:
        copy.start()

    barrier = pltpu.get_barrier_semaphore()
    for peer in peers:
        pl.semaphore_signal(barrier, inc=1, device_id={"tp": peer}, device_id_type=MESH)
    for d in range(1, n_sp):
        pl.semaphore_signal(barrier, inc=1, device_id={"sp": (sp + d) % n_sp}, device_id_type=MESH)
    pl.semaphore_wait(barrier, n_tp - 1 + n_sp - 1)

    def send(src, dst, ssem, rsem, device):
        return pltpu.make_async_remote_copy(
            src_ref=src, dst_ref=dst, send_sem=ssem, recv_sem=rsem, device_id=device, device_id_type=MESH
        )

    top, low = pl.ds(0, half), pl.ds(half, half)
    lat = []

    def send_rows(index, src, slot, piece, peer):
        copy = send(src, raw.at[slot, piece], lat_send.at[index], lat_recv.at[index], {"tp": peer})
        copy.start()
        lat.append(copy)

    send_rows(0, latent.at[top], 0, top, peers[0])
    send_rows(1, latent.at[low], 1, low, peers[1])
    send_rows(2, latent.at[low], 0, low, peers[0])
    send_rows(3, latent.at[top], 1, top, peers[1])

    act = jnp.concatenate([cond[...], cond_ctx[...]], axis=0).astype(jnp.float32)
    act = (act / (1.0 + jnp.exp(-act))).astype(jnp.bfloat16)
    act = jnp.concatenate([act, jnp.zeros((14, act.shape[1]), jnp.bfloat16)], axis=0)
    for i in range(3):
        local[i].wait()
    sums = [jnp.dot(act, mods_w[i], preferred_element_type=jnp.float32)[0:2] for i in range(3)]
    part[...] = jnp.concatenate(sums + [jnp.zeros((2, chunk), jnp.float32)], axis=0)
    pa = []
    for d in sp_order:
        copy = send(part, part_in.at[d - 1], pa_send.at[d - 1], pa_recv.at[d - 1], {"sp": (sp + d) % n_sp})
        copy.start()
        pa.append(copy)

    groups = tokens // GRID_W
    for i in range(2):
        for g in range(groups):
            rope[i, pl.ds(g * GRID_W, GRID_W), :] = (
                row_tab[i, pl.ds(sp * groups + g, 1), :] + col_tab[i, :, :]
            )
    local[4].wait()
    local[5].wait()
    wkv[...] = jnp.concatenate([wk[...], wv[...]], axis=1)

    total = part[...]
    for copy in pa:
        copy.wait_recv()
    for d in range(1, n_sp):
        total = total + part_in[d - 1]
    mods_all[tp] = total
    pb = []
    for i, peer in enumerate(peers):
        copy = send(mods_all.at[tp], mods_all.at[tp], pb_send.at[i], pb_recv.at[i], {"tp": peer})
        copy.start()
        pb.append(copy)
    lat[0].wait_recv()
    send_rows(4, raw.at[0, top], 2, top, peers[1])
    lat[1].wait_recv()
    send_rows(5, raw.at[1, low], 2, low, peers[0])

    for copy in pb:
        copy.wait_recv()
    gain = norm_gain[...].astype(jnp.float32)
    for j in range(n_tp):
        cols = pl.ds(j * chunk, chunk)
        block = mods_all[j]
        ab[0:2, cols] = gain[:, j * chunk : (j + 1) * chunk] * (1.0 + block[2:4])
        ab[2:4, cols] = block[0:2]

    lane = lax.broadcasted_iota(jnp.int32, (1, 2 * HD), 1)
    even = lane % 2 == 0
    left = lane < HD
    ones = (
        (lax.broadcasted_iota(jnp.int32, (2 * HD, 2 * HD), 0) < HD)
        == (lax.broadcasted_iota(jnp.int32, (2 * HD, 2 * HD), 1) < HD)
    ).astype(jnp.bfloat16)
    qg = jnp.concatenate([q_gain[...]] * 2, axis=1).astype(jnp.float32)
    kg = jnp.concatenate([k_gain[...]] * 2, axis=1).astype(jnp.float32)

    def modulated(block, row):
        values = block.astype(jnp.float32)
        scale = lax.rsqrt(jnp.mean(values * values, axis=-1, keepdims=True) + EPS)
        return (values * scale * ab[row : row + 1, :] + ab[row + 2 : row + 3, :]).astype(jnp.bfloat16)

    def headed(x, g):
        square = x * x
        high = square.astype(jnp.bfloat16)
        rest = (square - high.astype(jnp.float32)).astype(jnp.bfloat16)
        mean = (
            jnp.dot(high, ones, preferred_element_type=jnp.float32)
            + jnp.dot(rest, ones, preferred_element_type=jnp.float32)
        ) * (1.0 / HD)
        return x * lax.rsqrt(mean + EPS) * g

    def turned(x, cosine, sine):
        partner = jnp.where(even, pltpu.roll(x, 2 * HD - 1, 1), pltpu.roll(x, 1, 1))
        return x * cosine + partner * sine

    factor = LOG2E * HD ** (-0.5)

    def absorb_rows(block, owner):
        u = modulated(block, 0)
        where = pl.ds(pl.multiple_of(owner * rows, rows), rows)
        cosine, sine = rope[0, where, :], rope[1, where, :]
        kv = jnp.dot(u, wkv[...], preferred_element_type=jnp.float32)
        keys = turned(headed(kv, kg), cosine, sine)
        kv_all[0, where, :] = jnp.where(left, keys, kv).astype(jnp.bfloat16)
        raw_q = jnp.dot(u, wq[...], preferred_element_type=jnp.float32)
        for pair in range(group // 2):
            x = raw_q[:, pair * 2 * HD : (pair + 1) * 2 * HD]
            x = turned(headed(x, qg), cosine, sine).astype(jnp.bfloat16)
            q_tok[pair, where, :] = x.astype(jnp.float32) * factor

    local[3].wait()
    uc = modulated(context[...], 1)
    kvc = jnp.dot(uc, wkv[...], preferred_element_type=jnp.float32)
    kv_all[0, pl.ds(tokens, ctx_rows), :] = jnp.where(left, headed(kvc, kg), kvc).astype(jnp.bfloat16)
    local[6].wait()
    absorb_rows(latent[...], tp)
    lat[2].wait_recv()
    absorb_rows(raw[0], peers[0])
    lat[3].wait_recv()
    absorb_rows(raw[1], peers[1])
    lat[4].wait_recv()
    lat[5].wait_recv()
    absorb_rows(raw[2], peers[2])

    kvs = {}
    for d in sp_order:
        copy = send(kv_all.at[0], kv_all.at[d], kv_send.at[d - 1], kv_recv.at[d - 1], {"sp": (sp + d) % n_sp})
        copy.start()
        kvs[d] = copy

    blocks = tokens // QB
    for pair in range(group // 2):
        for tb in range(blocks):
            t = q_tok[pair, tb * QB : (tb + 1) * QB, :].T
            high = t.astype(jnp.bfloat16)
            rest = (t - high.astype(jnp.float32)).astype(jnp.bfloat16)
            none = jnp.zeros((HD, QB), jnp.bfloat16)
            for j in range(2):
                cut = slice(j * HD, (j + 1) * HD)
                q_t[tb * group + 2 * pair + j] = jnp.concatenate([high[cut], none, rest[cut], none], axis=0)
    v_t[HD:, :] = jnp.ones((v_t.shape[0] - HD, tokens), jnp.bfloat16)
    acc[...] = jnp.zeros_like(acc)
    m_st[...] = jnp.full(m_st.shape, -1e30, jnp.float32)
    n_q = blocks * group
    bufs = (s_a, s_b)

    def sweep(load, n_keys, lifted, done):
        chunks = n_keys // KB

        def scores(b, c, dst, top):
            piece = load(c)
            s = jnp.dot(
                jnp.concatenate([piece, piece], axis=1), q_t[b], preferred_element_type=jnp.float32
            )
            if lifted:
                s = s + lift[b % group] * LOG2E
            dst[c * KB : (c + 1) * KB, :] = s
            high = jnp.max(s.reshape(KB // 8, 8, QB), axis=0)
            return high if top is None else jnp.maximum(top, high)

        top = None
        for c in range(chunks):
            top = scores(0, c, bufs[0], top)
        for b in range(n_q):
            cur, nxt = bufs[b % 2], bufs[(b + 1) % 2]
            m_old = m_st[b]
            m = jnp.maximum(m_old, jnp.max(top, axis=0, keepdims=True))
            m_st[b] = m
            alpha = jnp.exp2(m_old - m)
            top, o = None, None
            for c in range(chunks):
                if b + 1 < n_q:
                    top = scores(b + 1, c, nxt, top)
                x = cur[c * KB : (c + 1) * KB, :].reshape(KB // 8, 8, QB) - m[None]
                p = jnp.exp2(x).reshape(KB, QB).astype(jnp.bfloat16)
                term = jnp.dot(v_t[:, c * KB : (c + 1) * KB], p, preferred_element_type=jnp.float32)
                o = term if o is None else o + term
            o = acc[b] * alpha[0:1] + o
            if done is None:
                acc[b] = o
            else:
                done(b, o)

    def kv_copy(d):
        return send(kv_all.at[0], kv_all.at[d], kv_send.at[d - 1], kv_recv.at[d - 1], {"sp": (sp + d) % n_sp})

    def slot_step(step, carry):
        d = jnp.where(step % 2 == 1, (step + 1) // 2, (n_sp - step // 2) % n_sp)

        @pl.when(step > 0)
        def _():
            kv_copy(d).wait_recv()

        kv_ctx[pl.ds(pl.multiple_of(step * ctx_rows, ctx_rows), ctx_rows), :] = kv_all[d, tokens:, :]
        for c in range(tokens // KB):
            v_t[:HD, c * KB : (c + 1) * KB] = kv_all[d, c * KB : (c + 1) * KB, :].T[HD:]
        sweep(lambda c: kv_all[d, c * KB : (c + 1) * KB, :], tokens, False, None)
        return carry

    lax.fori_loop(0, n_sp, slot_step, 0)

    finished = {}

    def done(b, o):
        finished[b % group] = (o[:HD] / o[HD : HD + 1]).astype(jnp.bfloat16).astype(jnp.float32)
        if b % group == group - 1:
            tb = b // group
            for pair in range(group // 2):
                both = jnp.concatenate([finished[2 * pair], finished[2 * pair + 1]], axis=0)
                o_tok[tb * QB : (tb + 1) * QB, pair * 2 * HD : (pair + 1) * 2 * HD] = both.T.astype(jnp.bfloat16)

    n_ctx = n_sp * ctx_rows
    for c in range(n_ctx // KB):
        v_t[:HD, c * KB : (c + 1) * KB] = kv_ctx[c * KB : (c + 1) * KB, :].T[HD:]
    sweep(lambda c: kv_ctx[c * KB : (c + 1) * KB, :], n_ctx, True, done)

    span = group * HD
    mine = pl.ds(pl.multiple_of(tp * span, span), span)
    o_copies = []
    for i, owner in enumerate(peers):
        where = pl.ds(pl.multiple_of(owner * rows, rows), rows)
        copy = send(o_tok.at[where], o_all.at[:, mine], o_ssem.at[i], o_rsem.at[i], {"tp": owner})
        copy.start()
        o_copies.append(copy)
    o_all[:, mine] = o_tok[pl.ds(pl.multiple_of(tp * rows, rows), rows), :]
    local[7].wait()
    for copy in o_copies:
        copy.wait_recv()

    for j in range(n_tp):
        cols = pl.ds(j * chunk, chunk)
        y = jnp.dot(o_all[...], wout[:, cols], preferred_element_type=jnp.float32)
        gate = mods_all[j, 4:5, :]
        out[:, cols] = (latent[:, cols].astype(jnp.float32) + gate * y).astype(jnp.bfloat16)

    for copy in lat + pa + pb + list(kvs.values()) + o_copies:
        copy.wait_send()


def on_device(n_sp, n_tp, latent, cond, cond_ctx, context, norm_gain, mod_shift, mod_scale, mod_gate,
              w_query, w_key, w_value, q_gain, k_gain, ctx_lift, w_out):
    _, rows, width = latent.shape
    tokens = rows * n_tp
    ctx_rows = context.shape[1]
    group = w_query.shape[1] // w_key.shape[1]
    keys = tokens + ctx_rows
    row_tab, col_tab = rope_tables(tokens * n_sp // GRID_W)
    chunk = mod_shift.shape[1]
    n_q = tokens // QB * group
    bf, f32 = jnp.bfloat16, jnp.float32
    vmem = pl.BlockSpec(memory_space=pltpu.VMEM)
    smem = pl.BlockSpec(memory_space=pltpu.SMEM)
    hbm = pl.BlockSpec(memory_space=pl.ANY)
    dma = pltpu.SemaphoreType.DMA
    out = pl.pallas_call(
        functools.partial(kernel, n_sp, n_tp, group),
        out_shape=jax.ShapeDtypeStruct((rows, width), bf),
        in_specs=[vmem] * 6 + [smem] + [vmem] * 2 + [hbm] * 8,
        out_specs=vmem,
        scratch_shapes=[
            pltpu.VMEM((ctx_rows, width), bf),
            pltpu.VMEM((3,) + mod_shift.shape, bf),
            pltpu.VMEM(w_query.shape, bf),
            pltpu.VMEM(w_key.shape, bf),
            pltpu.VMEM(w_value.shape, bf),
            pltpu.VMEM((width, 2 * HD), bf),
            pltpu.VMEM(w_out.shape, bf),
            pltpu.VMEM((n_tp - 1, rows, width), bf),
            pltpu.VMEM((8, chunk), f32),
            pltpu.VMEM((n_sp - 1, 8, chunk), f32),
            pltpu.VMEM((n_tp, 8, chunk), f32),
            pltpu.VMEM((8, width), f32),
            pltpu.VMEM((2, tokens, 2 * HD), f32),
            pltpu.VMEM((group // 2, tokens, 2 * HD), f32),
            pltpu.VMEM((n_q, 4 * HD, QB), bf),
            pltpu.VMEM((n_sp, keys, 2 * HD), bf),
            pltpu.VMEM((n_sp * ctx_rows, 2 * HD), bf),
            pltpu.VMEM((HD + 16, tokens), bf),
            pltpu.VMEM((tokens, QB), f32),
            pltpu.VMEM((tokens, QB), f32),
            pltpu.VMEM((n_q, HD + 16, QB), f32),
            pltpu.VMEM((n_q, 8, QB), f32),
            pltpu.VMEM((tokens, group * HD), bf),
            pltpu.VMEM((rows, n_tp * group * HD), bf),
            dma((8,)),
            dma((6,)), dma((6,)),
            dma((n_sp - 1,)), dma((n_sp - 1,)),
            dma((n_tp - 1,)), dma((n_tp - 1,)),
            dma((n_sp - 1,)), dma((n_sp - 1,)),
            dma((n_tp - 1,)), dma((n_tp - 1,)),
        ],
        compiler_params=pltpu.CompilerParams(
            collective_id=0, has_side_effects=True, vmem_limit_bytes=60 * 1024 * 1024
        ),
    )(
        latent[0], cond, cond_ctx[None], norm_gain[None], q_gain[None], k_gain[None], ctx_lift,
        jnp.asarray(row_tab), jnp.asarray(col_tab),
        context[0], mod_shift, mod_scale, mod_gate, w_query, w_key, w_value, w_out,
    )
    return out[None]


def solution(mesh):
    placed = (
        P("dp", ("sp", "tp"), None),
        P("dp", "sp"),
        P("sp"),
        P("dp", "sp", None),
        P(),
        P("sp", "tp"),
        P("sp", "tp"),
        P("sp", "tp"),
        P(None, "tp"),
        P(None, "tp"),
        P(None, "tp"),
        P(),
        P(),
        P("tp"),
        P(),
    )
    return jax.shard_map(
        functools.partial(on_device, mesh.shape["sp"], mesh.shape["tp"]),
        mesh=mesh,
        in_specs=placed,
        out_specs=P("dp", ("sp", "tp"), None),
        check_vma=False,
    )
```

```python
import functools

import jax
import jax.numpy as jnp
import numpy as np
from jax import lax
from jax.experimental import pallas as pl
from jax.experimental.pallas import tpu as pltpu
from jax.sharding import PartitionSpec as P

HD = 64
GRID_W = 128
EPS = 1e-06
THETA = 10000.0
MESH = pl.DeviceIdType.MESH
LOG2E = 1.4426950408889634
QB = 256
KB = 256
TILE = 128

PAIRS = (
    ((0, 0), (3, 0)), ((1, 0), (0, 3)), ((0, 1), (2, 0)), ((3, 3), (3, 1)),
    ((1, 3), (1, 1)), ((2, 3), (2, 1)), ((0, 2), (3, 2)), ((1, 2), (2, 2)),
)
ONWARD = {
    (0, 0): ((0, 1, (3, 0)), (0, -1, (1, 0)), (1, 1, (0, 3)), (1, -1, (0, 1))),
    (3, 0): ((0, 1, (2, 0)), (1, 1, (3, 3)), (1, -1, (3, 1))),
    (1, 0): ((1, 1, (1, 3)), (1, -1, (1, 1))),
    (2, 0): ((1, 1, (2, 3)), (1, -1, (2, 1))),
    (0, 3): ((1, 1, (0, 2)),),
    (1, 3): ((1, 1, (1, 2)),),
    (3, 1): ((1, -1, (3, 2)),),
    (2, 1): ((1, -1, (2, 2)),),
}


def slot_of(place):
    return place[0] * 4 + place[1]


def pick(step, values):
    chosen = values[0]
    for i, value in enumerate(values[1:], 1):
        chosen = jnp.where(step == i, value, chosen)
    return chosen


def rope_tables(grid_rows):
    n = HD // 4
    inverse = (np.float32(THETA) ** (-np.arange(n, dtype=np.float32) / np.float32(n))).astype(np.float32)

    def table(count, low):
        angles = (np.arange(count, dtype=np.float32)[:, None] * inverse).astype(np.float32)
        zero = np.zeros((count, 2 * n), np.float32)
        sign = np.tile(np.array([-1.0, 1.0], np.float32), n)
        c = np.repeat(np.cos(angles.astype(np.float64)), 2, axis=1).astype(np.float32)
        s = np.repeat(np.sin(angles.astype(np.float64)), 2, axis=1).astype(np.float32) * sign
        parts = ([c, zero], [s, zero]) if low else ([zero, c], [zero, s])
        return [np.tile(np.concatenate(p, axis=1), (1, 2)) for p in parts]

    return np.stack(table(grid_rows, True)), np.stack(table(GRID_W, False))


def kernel(
    n_sp, n_tp, group,
    latent, cond, cond_ctx, norm_gain, q_gain, k_gain, lift, row_tab, col_tab,
    context_h, mshift_h, mscale_h, mgate_h, wq_h, wk_h, wv_h, wout_h,
    out,
    context, mods_w, wq, wkv, wout,
    raw, part, part_in, mods_all, ab, rope, u_buf, q_t, kv1, kv2, kv_ctx, v_t, s_a, s_b, acc, m_st, o_tok, o_all,
    local_sem, lat_send, lat_recv, pa_send, pa_recv, pb_send, pb_recv, kv_send, kv_recv, o_ssem, o_rsem,
):
    rows = latent.shape[0]
    half = rows // 2
    width = latent.shape[1]
    chunk = width // n_tp
    tokens = rows * n_tp
    share = tokens // 2
    ctx_rows = context.shape[0]
    sp = lax.axis_index("sp")
    tp = lax.axis_index("tp")
    dp = lax.axis_index("dp")
    left_tp, right_tp, far_tp = (tp + n_tp - 1) % n_tp, (tp + 1) % n_tp, (tp + 2) % n_tp
    peers = (left_tp, right_tp, far_tp)
    sp_order = sorted(range(1, n_sp), key=lambda d: min(d, n_sp - d))

    local = [
        pltpu.make_async_copy(src, dst, local_sem.at[i])
        for i, (src, dst) in enumerate(
            (
                (mshift_h, mods_w.at[0]),
                (mscale_h, mods_w.at[1]),
                (mgate_h, mods_w.at[2]),
                (context_h, context),
                (wk_h, wkv.at[0:HD]),
                (wv_h, wkv.at[HD : 2 * HD]),
                (wq_h, wq),
                (wout_h, wout),
            )
        )
    ]
    for copy in local:
        copy.start()

    barrier = pltpu.get_barrier_semaphore()
    for peer in peers:
        pl.semaphore_signal(barrier, inc=1, device_id={"tp": peer}, device_id_type=MESH)
    for d in range(1, n_sp):
        pl.semaphore_signal(barrier, inc=1, device_id={"sp": (sp + d) % n_sp}, device_id_type=MESH)
    pl.semaphore_wait(barrier, n_tp - 1 + n_sp - 1)

    def send(src, dst, ssem, rsem, device):
        return pltpu.make_async_remote_copy(
            src_ref=src, dst_ref=dst, send_sem=ssem, recv_sem=rsem, device_id=device, device_id_type=MESH
        )

    top, low = pl.ds(0, half), pl.ds(half, half)
    lat = []

    def send_rows(index, src, slot, piece, peer):
        copy = send(src, raw.at[slot, piece], lat_send.at[index], lat_recv.at[index], {"tp": peer})
        copy.start()
        lat.append(copy)

    send_rows(0, latent.at[top], 0, top, right_tp)
    send_rows(1, latent.at[top], 1, top, left_tp)

    act = jnp.concatenate([cond[...], cond_ctx[...]], axis=0).astype(jnp.float32)
    act = (act / (1.0 + jnp.exp(-act))).astype(jnp.bfloat16)
    act = jnp.concatenate([act, jnp.zeros((14, act.shape[1]), jnp.bfloat16)], axis=0)
    for i in range(3):
        local[i].wait()
    sums = [jnp.dot(act, mods_w[i], preferred_element_type=jnp.float32)[0:2] for i in range(3)]
    part[...] = jnp.concatenate(sums + [jnp.zeros((2, chunk), jnp.float32)], axis=0)
    pa = []
    for d in sp_order:
        copy = send(part, part_in.at[d - 1], pa_send.at[d - 1], pa_recv.at[d - 1], {"sp": (sp + d) % n_sp})
        copy.start()
        pa.append(copy)

    groups = tokens // GRID_W
    for i in range(2):
        for g in range(groups):
            rope[i, pl.ds(g * GRID_W, GRID_W), :] = (
                row_tab[i, pl.ds(sp * groups + g, 1), :] + col_tab[i, :, :]
            )

    total = part[...]
    for copy in pa:
        copy.wait_recv()
    for d in range(1, n_sp):
        total = total + part_in[d - 1]
    mods_all[tp] = total
    pb = []
    for i, peer in enumerate((far_tp, left_tp, right_tp)):
        copy = send(mods_all.at[tp], mods_all.at[tp], pb_send.at[i], pb_recv.at[i], {"tp": peer})
        copy.start()
        pb.append(copy)
    send_rows(2, latent.at[low], 0, low, right_tp)
    send_rows(3, latent.at[low], 1, low, left_tp)

    for i, peer in enumerate((far_tp, left_tp, right_tp)):
        pb[i].wait_recv()
    for j in range(n_tp):
        block = mods_all[j]
        for i in range(chunk // TILE):
            at = j * chunk + i * TILE
            gain = norm_gain[at // TILE : at // TILE + 1, :].astype(jnp.float32)
            ab[0:2, at : at + TILE] = gain * (1.0 + block[2:4, i * TILE : (i + 1) * TILE])
        ab[2:4, pl.ds(j * chunk, chunk)] = block[0:2]

    lane = lax.broadcasted_iota(jnp.int32, (1, 2 * HD), 1)
    even = lane % 2 == 0
    left = lane < HD
    ones = (
        (lax.broadcasted_iota(jnp.int32, (2 * HD, 2 * HD), 0) < HD)
        == (lax.broadcasted_iota(jnp.int32, (2 * HD, 2 * HD), 1) < HD)
    ).astype(jnp.bfloat16)
    qg = jnp.concatenate([q_gain[...]] * 2, axis=1).astype(jnp.float32)
    kg = jnp.concatenate([k_gain[...]] * 2, axis=1).astype(jnp.float32)
    factor = LOG2E * HD ** (-0.5)

    def modulated(block, row):
        values = block.astype(jnp.float32)
        scale = lax.rsqrt(jnp.mean(values * values, axis=-1, keepdims=True) + EPS)
        return (values * scale * ab[row : row + 1, :] + ab[row + 2 : row + 3, :]).astype(jnp.bfloat16)

    def headed(x, g):
        square = x * x
        high = square.astype(jnp.bfloat16)
        rest = (square - high.astype(jnp.float32)).astype(jnp.bfloat16)
        mean = (
            jnp.dot(high, ones, preferred_element_type=jnp.float32)
            + jnp.dot(rest, ones, preferred_element_type=jnp.float32)
        ) * (1.0 / HD)
        return x * lax.rsqrt(mean + EPS) * g

    def turned(x, cosine, sine):
        partner = jnp.where(even, pltpu.roll(x, 2 * HD - 1, 1), pltpu.roll(x, 1, 1))
        return x * cosine + partner * sine

    def key_value(u):
        return lax.dot_general(u, wkv[...], (((1,), (1,)), ((), ())), preferred_element_type=jnp.float32)

    def angles(owner, start, count):
        where = pl.ds(pl.multiple_of(owner * rows + start, half), count)
        return rope[0, where, :], rope[1, where, :]

    def absorb_keys(block, owner, start, kv, offset):
        count = block.shape[0]
        u = modulated(block, 0)
        u_buf[offset : offset + count, :] = u
        cosine, sine = angles(owner, start, count)
        x = key_value(u)
        kv[0, offset : offset + count, :] = jnp.where(
            left, turned(headed(x, kg), cosine, sine), x
        ).astype(jnp.bfloat16)

    def absorb_queries(pieces, first):
        tables = [angles(*piece) for piece in pieces]
        cosine = jnp.concatenate([t[0] for t in tables], axis=0)
        sine = jnp.concatenate([t[1] for t in tables], axis=0)
        raw_q = jnp.dot(u_buf[...], wq[...], preferred_element_type=jnp.float32)
        none = jnp.zeros((HD, QB), jnp.bfloat16)
        for pair in range(group // 2):
            x = raw_q[:, pair * 2 * HD : (pair + 1) * 2 * HD]
            x = turned(headed(x, qg), cosine, sine).astype(jnp.bfloat16).astype(jnp.float32) * factor
            for tile in range(tiles):
                t = x[tile * TILE : (tile + 1) * TILE, :].T
                t = jnp.concatenate([t[:HD], t[HD:]], axis=1)
                high = t.astype(jnp.bfloat16)
                rest = (t - high.astype(jnp.float32)).astype(jnp.bfloat16)
                q_t[first + pair * tiles + tile] = jnp.concatenate([high, none, rest, none], axis=0)

    side = int(round(n_sp ** 0.5))
    y, z = sp % side, sp // side

    def neighbour(axis, step):
        along_y = z * side + (y + step + side) % side
        along_z = (z + step + side) % side * side + y
        return jnp.where(dp == axis, along_y, along_z)

    flights = [(place, hop) for place in ONWARD for hop in ONWARD[place]]

    def flight(index, which, kv):
        place, (axis, step, target) = flights[index]
        return send(
            kv.at[slot_of(place)], kv.at[slot_of(target)],
            kv_send.at[which, index], kv_recv.at[which, slot_of(target)],
            {"sp": neighbour(axis, step)},
        )

    def pass_on(place, which, kv):
        for index in range(len(flights)):
            if flights[index][0] == place:
                flight(index, which, kv).start()

    def arrived(place, which, kv):
        for index in range(len(flights)):
            if flights[index][1][2] == place:
                flight(index, which, kv).wait_recv()

    tiles = share // TILE
    n_half = tiles * group // 2
    bufs = (s_a, s_b)

    def sweep(load, n_keys, order, lifted, done):
        chunks = n_keys // KB

        def scores(b, c, dst, top):
            piece = load(c)
            s = jnp.dot(
                jnp.concatenate([piece, piece], axis=1), q_t[b], preferred_element_type=jnp.float32
            )
            if lifted:
                pair = b % n_half // tiles
                wide = lax.broadcasted_iota(jnp.int32, (1, QB), 1)
                s = s + jnp.where(wide < TILE, lift[2 * pair], lift[2 * pair + 1]) * LOG2E
            dst[c * KB : (c + 1) * KB, :] = s
            high = jnp.max(s.reshape(KB // 8, 8, QB), axis=0)
            return high if top is None else jnp.maximum(top, high)

        top = None
        for c in range(chunks):
            top = scores(order[0], c, bufs[0], top)
        for i, b in enumerate(order):
            cur, nxt = bufs[i % 2], bufs[(i + 1) % 2]
            m_old = m_st[b]
            m = jnp.maximum(m_old, jnp.max(top, axis=0, keepdims=True))
            m_st[b] = m
            alpha = jnp.exp2(m_old - m)
            top, o = None, None
            for c in range(chunks):
                if i + 1 < len(order):
                    top = scores(order[i + 1], c, nxt, top)
                x = cur[c * KB : (c + 1) * KB, :].reshape(KB // 8, 8, QB) - m[None]
                p = jnp.exp2(x).reshape(KB, QB).astype(jnp.bfloat16)
                term = jnp.dot(v_t[:, c * KB : (c + 1) * KB], p, preferred_element_type=jnp.float32)
                o = term if o is None else o + term
            o = acc[b] * alpha[0:1] + o
            if done is None:
                acc[b] = o
            else:
                done(b, o)

    def pair_sweep(step, order, which, kv):
        if which is not None:
            for k, places in enumerate(PAIRS):
                @pl.when(step == k)
                def _(k=k, places=places):
                    for place in places:
                        if place != (0, 0):
                            arrived(place, which, kv)
                            pass_on(place, which, kv)

        ids = [pick(step, [slot_of(places[i]) for places in PAIRS]) for i in range(2)]

        def tile_at(t):
            return kv[ids[t // tiles], t % tiles * TILE : (t % tiles + 1) * TILE, :]

        for t in range(2 * tiles):
            v_t[:HD, t * TILE : (t + 1) * TILE] = tile_at(t).T[HD:]
        per = KB // TILE
        sweep(
            lambda c: jnp.concatenate([tile_at(c * per + i) for i in range(per)], axis=0),
            2 * share, order, False, None,
        )

    v_t[HD:, :] = jnp.ones((v_t.shape[0] - HD, v_t.shape[1]), jnp.bfloat16)
    acc[...] = jnp.zeros_like(acc)
    m_st[...] = jnp.full(m_st.shape, -1e30, jnp.float32)

    first_half, second_half = list(range(n_half)), list(range(n_half, 2 * n_half))
    local[4].wait()
    local[5].wait()
    absorb_keys(latent[...], tp, 0, kv1, 0)
    lat[0].wait_recv()
    send_rows(4, raw.at[0, top], 2, top, right_tp)
    absorb_keys(raw[0, top, :], left_tp, 0, kv1, rows)
    lat[1].wait_recv()
    absorb_keys(raw[1, top, :], right_tp, 0, kv1, rows + half)
    pass_on((0, 0), 0, kv1)
    local[6].wait()
    absorb_queries([(tp, 0, rows), (left_tp, 0, half), (right_tp, 0, half)], 0)

    last_rows = send(raw.at[1, low], raw.at[2, low], lat_send.at[5], lat_recv.at[5], {"tp": left_tp})

    def one(step, carry):
        @pl.when(step == 1)
        def _():
            lat[3].wait_recv()
            last_rows.start()

        pair_sweep(step, first_half, 0, kv1)
        return carry

    lax.fori_loop(0, len(PAIRS), one, 0)

    local[3].wait()
    x = key_value(modulated(context[...], 1))
    kv2[0, share : share + ctx_rows, :] = jnp.where(left, headed(x, kg), x).astype(jnp.bfloat16)
    lat[2].wait_recv()
    absorb_keys(raw[0, low, :], left_tp, half, kv2, 0)
    absorb_keys(raw[1, low, :], right_tp, half, kv2, half)
    lat[4].wait_recv()
    last_rows.wait_recv()
    absorb_keys(raw[2], far_tp, 0, kv2, rows)
    pass_on((0, 0), 1, kv2)
    absorb_queries([(left_tp, half, half), (right_tp, half, half), (far_tp, 0, rows)], n_half)

    def two(step, carry):
        pair_sweep(step, second_half, None, kv1)
        return carry

    lax.fori_loop(0, len(PAIRS), two, 0)

    def three(step, carry):
        pair_sweep(step, first_half + second_half, 1, kv2)
        return carry

    lax.fori_loop(0, len(PAIRS), three, 0)

    def done(b, o):
        o = (o[:HD] / o[HD : HD + 1]).astype(jnp.bfloat16).astype(jnp.float32)
        both = jnp.concatenate([o[:, :TILE], o[:, TILE:]], axis=0)
        pair, tile = b % n_half // tiles, b % n_half % tiles
        at = b // n_half * share + tile * TILE
        o_tok[at : at + TILE, pair * 2 * HD : (pair + 1) * 2 * HD] = both.T.astype(jnp.bfloat16)

    for slot in range(n_sp):
        kv_ctx[slot * ctx_rows : (slot + 1) * ctx_rows, :] = kv2[slot, share:, :]
    n_ctx = n_sp * ctx_rows
    for t in range(n_ctx // TILE):
        v_t[:HD, t * TILE : (t + 1) * TILE] = kv_ctx[t * TILE : (t + 1) * TILE, :].T[HD:]
    sweep(lambda c: kv_ctx[c * KB : (c + 1) * KB, :], n_ctx, second_half + first_half, True, done)

    span = group * HD
    mine = pl.ds(pl.multiple_of(tp * span, span), span)
    o_copies = []
    for i, (at, count, owner, start) in enumerate(
        (
            (share + rows, rows, far_tp, 0),
            (share, half, left_tp, half),
            (share + half, half, right_tp, half),
            (rows, half, left_tp, 0),
            (rows + half, half, right_tp, 0),
        )
    ):
        copy = send(
            o_tok.at[at : at + count], o_all.at[start : start + count, mine],
            o_ssem.at[i], o_rsem.at[i], {"tp": owner},
        )
        copy.start()
        o_copies.append(copy)
    o_all[:, mine] = o_tok[0:rows, :]
    local[7].wait()
    for copy in o_copies:
        copy.wait_recv()

    for j in range(n_tp):
        cols = pl.ds(j * chunk, chunk)
        y_j = jnp.dot(o_all[...], wout[:, cols], preferred_element_type=jnp.float32)
        gate = mods_all[j, 4:5, :]
        out[:, cols] = (latent[:, cols].astype(jnp.float32) + gate * y_j).astype(jnp.bfloat16)

    for copy in lat + [last_rows] + pa + pb + o_copies:
        copy.wait_send()
    for index in range(len(flights)):
        flight(index, 0, kv1).wait_send()
        flight(index, 1, kv2).wait_send()


def on_device(n_sp, n_tp, latent, cond, cond_ctx, context, norm_gain, mod_shift, mod_scale, mod_gate,
              w_query, w_key, w_value, q_gain, k_gain, ctx_lift, w_out):
    _, rows, width = latent.shape
    tokens = rows * n_tp
    ctx_rows = context.shape[1]
    group = w_query.shape[1] // w_key.shape[1]
    keys = tokens + ctx_rows
    row_tab, col_tab = rope_tables(tokens * n_sp // GRID_W)
    chunk = mod_shift.shape[1]
    share = tokens // 2
    n_q = tokens // TILE * group // 2
    bf, f32 = jnp.bfloat16, jnp.float32
    vmem = pl.BlockSpec(memory_space=pltpu.VMEM)
    smem = pl.BlockSpec(memory_space=pltpu.SMEM)
    hbm = pl.BlockSpec(memory_space=pl.ANY)
    dma = pltpu.SemaphoreType.DMA
    out = pl.pallas_call(
        functools.partial(kernel, n_sp, n_tp, group),
        out_shape=jax.ShapeDtypeStruct((rows, width), bf),
        in_specs=[vmem] * 6 + [smem] + [vmem] * 2 + [hbm] * 8,
        out_specs=vmem,
        scratch_shapes=[
            pltpu.VMEM((ctx_rows, width), bf),
            pltpu.VMEM((3,) + mod_shift.shape, bf),
            pltpu.VMEM(w_query.shape, bf),
            pltpu.VMEM((2 * HD, width), bf),
            pltpu.VMEM(w_out.shape, bf),
            pltpu.VMEM((n_tp - 1, rows, width), bf),
            pltpu.VMEM((8, chunk), f32),
            pltpu.VMEM((n_sp - 1, 8, chunk), f32),
            pltpu.VMEM((n_tp, 8, chunk), f32),
            pltpu.VMEM((8, width), f32),
            pltpu.VMEM((2, tokens, 2 * HD), f32),
            pltpu.VMEM((share, width), bf),
            pltpu.VMEM((n_q, 4 * HD, QB), bf),
            pltpu.VMEM((n_sp, share, 2 * HD), bf),
            pltpu.VMEM((n_sp, share + ctx_rows, 2 * HD), bf),
            pltpu.VMEM((n_sp * ctx_rows, 2 * HD), bf),
            pltpu.VMEM((HD + 16, tokens), bf),
            pltpu.VMEM((tokens, QB), f32),
            pltpu.VMEM((tokens, QB), f32),
            pltpu.VMEM((n_q, HD + 16, QB), f32),
            pltpu.VMEM((n_q, 8, QB), f32),
            pltpu.VMEM((tokens, group * HD), bf),
            pltpu.VMEM((rows, n_tp * group * HD), bf),
            dma((8,)),
            dma((6,)), dma((6,)),
            dma((n_sp - 1,)), dma((n_sp - 1,)),
            dma((n_tp - 1,)), dma((n_tp - 1,)),
            dma((2, n_sp - 1)), dma((2, n_sp)),
            dma((5,)), dma((5,)),
        ],
        compiler_params=pltpu.CompilerParams(
            collective_id=0, has_side_effects=True, vmem_limit_bytes=60 * 1024 * 1024
        ),
    )(
        latent[0], cond, cond_ctx[None], norm_gain.reshape(width // TILE, TILE), q_gain[None], k_gain[None], ctx_lift,
        jnp.asarray(row_tab), jnp.asarray(col_tab),
        context[0], mod_shift, mod_scale, mod_gate, w_query, w_key.T, w_value.T, w_out,
    )
    return out[None]


def solution(mesh):
    placed = (
        P("dp", ("sp", "tp"), None),
        P("dp", "sp"),
        P("sp"),
        P("dp", "sp", None),
        P(),
        P("sp", "tp"),
        P("sp", "tp"),
        P("sp", "tp"),
        P(None, "tp"),
        P(None, "tp"),
        P(None, "tp"),
        P(),
        P(),
        P("tp"),
        P(),
    )
    return jax.shard_map(
        functools.partial(on_device, mesh.shape["sp"], mesh.shape["tp"]),
        mesh=mesh,
        in_specs=placed,
        out_specs=P("dp", ("sp", "tp"), None),
        check_vma=False,
    )
```

```python
import functools

import jax
import jax.numpy as jnp
import numpy as np
from jax import lax
from jax.experimental import pallas as pl
from jax.experimental.pallas import tpu as pltpu
from jax.sharding import PartitionSpec as P

HD = 64
GRID_W = 128
EPS = 1e-06
THETA = 10000.0
MESH = pl.DeviceIdType.MESH
LOG2E = 1.4426950408889634
QB = 256
KB = 256
TILE = 128

GROUPS = (
    ((0, 0), (3, 0), (1, 0), (0, 3)),
    ((0, 1), (2, 0), (3, 3), (3, 1)),
    ((1, 3), (1, 1), (2, 3), (2, 1)),
    ((0, 2), (3, 2), (1, 2), (2, 2)),
)
AHEAD = 3
ONWARD = {
    (0, 0): ((0, 1, (3, 0)), (0, -1, (1, 0)), (1, 1, (0, 3)), (1, -1, (0, 1))),
    (3, 0): ((0, 1, (2, 0)), (1, 1, (3, 3)), (1, -1, (3, 1))),
    (1, 0): ((1, 1, (1, 3)), (1, -1, (1, 1))),
    (2, 0): ((1, 1, (2, 3)), (1, -1, (2, 1))),
    (0, 3): ((1, 1, (0, 2)),),
    (1, 3): ((1, 1, (1, 2)),),
    (3, 1): ((1, -1, (3, 2)),),
    (2, 1): ((1, -1, (2, 2)),),
}


def slot_of(place):
    return place[0] * 4 + place[1]


def pick(step, values):
    chosen = values[0]
    for i, value in enumerate(values[1:], 1):
        chosen = jnp.where(step == i, value, chosen)
    return chosen


def rope_tables(grid_rows):
    n = HD // 4
    inverse = (np.float32(THETA) ** (-np.arange(n, dtype=np.float32) / np.float32(n))).astype(np.float32)

    def table(count, low):
        angles = (np.arange(count, dtype=np.float32)[:, None] * inverse).astype(np.float32)
        zero = np.zeros((count, 2 * n), np.float32)
        sign = np.tile(np.array([-1.0, 1.0], np.float32), n)
        c = np.repeat(np.cos(angles.astype(np.float64)), 2, axis=1).astype(np.float32)
        s = np.repeat(np.sin(angles.astype(np.float64)), 2, axis=1).astype(np.float32) * sign
        parts = ([c, zero], [s, zero]) if low else ([zero, c], [zero, s])
        return [np.tile(np.concatenate(p, axis=1), (1, 2)) for p in parts]

    return np.stack(table(grid_rows, True)), np.stack(table(GRID_W, False))


def kernel(
    n_sp, n_tp, group,
    latent, cond, cond_ctx, norm_gain, q_gain, k_gain, lift, row_tab, col_tab,
    context_h, mshift_h, mscale_h, mgate_h, wq_h, wk_h, wv_h, wout_h,
    out,
    context, mods_w, wq, wkv, wout,
    raw, part, part_in, mods_all, ab, rope, u_buf, q_t, kv1, kv2, kv_ctx, v_t, s_buf, acc, m_st, o_tok, o_all,
    local_sem, lat_send, lat_recv, pa_send, pa_recv, pb_send, pb_recv, kv_send, kv_recv, o_ssem, o_rsem,
):
    rows = latent.shape[0]
    half = rows // 2
    width = latent.shape[1]
    chunk = width // n_tp
    tokens = rows * n_tp
    share = tokens // 2
    ctx_rows = context.shape[0]
    sp = lax.axis_index("sp")
    tp = lax.axis_index("tp")
    dp = lax.axis_index("dp")
    left_tp, right_tp, far_tp = (tp + n_tp - 1) % n_tp, (tp + 1) % n_tp, (tp + 2) % n_tp
    peers = (left_tp, right_tp, far_tp)
    sp_order = sorted(range(1, n_sp), key=lambda d: min(d, n_sp - d))

    local = [
        pltpu.make_async_copy(src, dst, local_sem.at[i])
        for i, (src, dst) in enumerate(
            (
                (mshift_h, mods_w.at[0]),
                (mscale_h, mods_w.at[1]),
                (mgate_h, mods_w.at[2]),
                (context_h, context),
                (wk_h, wkv.at[0:HD]),
                (wv_h, wkv.at[HD : 2 * HD]),
                (wq_h, wq),
                (wout_h, wout),
            )
        )
    ]
    for copy in local:
        copy.start()

    barrier = pltpu.get_barrier_semaphore()
    for peer in peers:
        pl.semaphore_signal(barrier, inc=1, device_id={"tp": peer}, device_id_type=MESH)
    for d in range(1, n_sp):
        pl.semaphore_signal(barrier, inc=1, device_id={"sp": (sp + d) % n_sp}, device_id_type=MESH)
    pl.semaphore_wait(barrier, n_tp - 1 + n_sp - 1)

    def send(src, dst, ssem, rsem, device):
        return pltpu.make_async_remote_copy(
            src_ref=src, dst_ref=dst, send_sem=ssem, recv_sem=rsem, device_id=device, device_id_type=MESH
        )

    top, low = pl.ds(0, half), pl.ds(half, half)
    lat = []

    def send_rows(index, src, slot, piece, peer):
        copy = send(src, raw.at[slot, piece], lat_send.at[index], lat_recv.at[index], {"tp": peer})
        copy.start()
        lat.append(copy)

    send_rows(0, latent.at[top], 0, top, right_tp)
    send_rows(1, latent.at[top], 1, top, left_tp)

    act = jnp.concatenate([cond[...], cond_ctx[...]], axis=0).astype(jnp.float32)
    act = (act / (1.0 + jnp.exp(-act))).astype(jnp.bfloat16)
    act = jnp.concatenate([act, jnp.zeros((14, act.shape[1]), jnp.bfloat16)], axis=0)
    for i in range(3):
        local[i].wait()
    sums = [jnp.dot(act, mods_w[i], preferred_element_type=jnp.float32)[0:2] for i in range(3)]
    part[...] = jnp.concatenate(sums + [jnp.zeros((2, chunk), jnp.float32)], axis=0)
    pa = []
    for d in sp_order:
        copy = send(part, part_in.at[d - 1], pa_send.at[d - 1], pa_recv.at[d - 1], {"sp": (sp + d) % n_sp})
        copy.start()
        pa.append(copy)

    groups = tokens // GRID_W
    for i in range(2):
        for g in range(groups):
            rope[i, pl.ds(g * GRID_W, GRID_W), :] = (
                row_tab[i, pl.ds(sp * groups + g, 1), :] + col_tab[i, :, :]
            )

    total = part[...]
    for copy in pa:
        copy.wait_recv()
    for d in range(1, n_sp):
        total = total + part_in[d - 1]
    mods_all[tp] = total
    pb = []
    for i, peer in enumerate((far_tp, left_tp, right_tp)):
        copy = send(mods_all.at[tp], mods_all.at[tp], pb_send.at[i], pb_recv.at[i], {"tp": peer})
        copy.start()
        pb.append(copy)
    send_rows(2, latent.at[low], 0, low, right_tp)
    send_rows(3, latent.at[low], 1, low, left_tp)

    for i, peer in enumerate((far_tp, left_tp, right_tp)):
        pb[i].wait_recv()
    for j in range(n_tp):
        block = mods_all[j]
        for i in range(chunk // TILE):
            at = j * chunk + i * TILE
            gain = norm_gain[at // TILE : at // TILE + 1, :].astype(jnp.float32)
            ab[0:2, at : at + TILE] = gain * (1.0 + block[2:4, i * TILE : (i + 1) * TILE])
        ab[2:4, pl.ds(j * chunk, chunk)] = block[0:2]

    lane = lax.broadcasted_iota(jnp.int32, (1, 2 * HD), 1)
    even = lane % 2 == 0
    left = lane < HD
    ones = (
        (lax.broadcasted_iota(jnp.int32, (2 * HD, 2 * HD), 0) < HD)
        == (lax.broadcasted_iota(jnp.int32, (2 * HD, 2 * HD), 1) < HD)
    ).astype(jnp.bfloat16)
    qg = jnp.concatenate([q_gain[...]] * 2, axis=1).astype(jnp.float32)
    kg = jnp.concatenate([k_gain[...]] * 2, axis=1).astype(jnp.float32)
    factor = LOG2E * HD ** (-0.5)

    def modulated(block, row):
        values = block.astype(jnp.float32)
        scale = lax.rsqrt(jnp.mean(values * values, axis=-1, keepdims=True) + EPS)
        return (values * scale * ab[row : row + 1, :] + ab[row + 2 : row + 3, :]).astype(jnp.bfloat16)

    def headed(x, g):
        square = x * x
        high = square.astype(jnp.bfloat16)
        rest = (square - high.astype(jnp.float32)).astype(jnp.bfloat16)
        mean = (
            jnp.dot(high, ones, preferred_element_type=jnp.float32)
            + jnp.dot(rest, ones, preferred_element_type=jnp.float32)
        ) * (1.0 / HD)
        return x * lax.rsqrt(mean + EPS) * g

    def turned(x, cosine, sine):
        partner = jnp.where(even, pltpu.roll(x, 2 * HD - 1, 1), pltpu.roll(x, 1, 1))
        return x * cosine + partner * sine

    def key_value(u):
        return lax.dot_general(u, wkv[...], (((1,), (1,)), ((), ())), preferred_element_type=jnp.float32)

    def angles(owner, start, count):
        where = pl.ds(pl.multiple_of(owner * rows + start, half), count)
        return rope[0, where, :], rope[1, where, :]

    def absorb_keys(block, owner, start, kv, offset):
        count = block.shape[0]
        u = modulated(block, 0)
        u_buf[offset : offset + count, :] = u
        cosine, sine = angles(owner, start, count)
        x = key_value(u)
        kv[0, offset : offset + count, :] = jnp.where(
            left, turned(headed(x, kg), cosine, sine), x
        ).astype(jnp.bfloat16)

    def absorb_queries(pieces, first):
        tables = [angles(*piece) for piece in pieces]
        cosine = jnp.concatenate([t[0] for t in tables], axis=0)
        sine = jnp.concatenate([t[1] for t in tables], axis=0)
        raw_q = jnp.dot(u_buf[...], wq[...], preferred_element_type=jnp.float32)
        none = jnp.zeros((HD, QB), jnp.bfloat16)
        for pair in range(group // 2):
            x = raw_q[:, pair * 2 * HD : (pair + 1) * 2 * HD]
            x = turned(headed(x, qg), cosine, sine).astype(jnp.bfloat16).astype(jnp.float32) * factor
            for tile in range(tiles):
                t = x[tile * TILE : (tile + 1) * TILE, :].T
                t = jnp.concatenate([t[:HD], t[HD:]], axis=1)
                high = t.astype(jnp.bfloat16)
                rest = (t - high.astype(jnp.float32)).astype(jnp.bfloat16)
                q_t[first + pair * tiles + tile] = jnp.concatenate([high, none, rest, none], axis=0)

    side = int(round(n_sp ** 0.5))
    y, z = sp % side, sp // side

    def neighbour(axis, step):
        along_y = z * side + (y + step + side) % side
        along_z = (z + step + side) % side * side + y
        return jnp.where(dp == axis, along_y, along_z)

    flights = [(place, hop) for place in ONWARD for hop in ONWARD[place]]

    def flight(index, which, kv):
        place, (axis, step, target) = flights[index]
        return send(
            kv.at[slot_of(place)], kv.at[slot_of(target)],
            kv_send.at[which, index], kv_recv.at[which, slot_of(target)],
            {"sp": neighbour(axis, step)},
        )

    def pass_on(place, which, kv):
        for index in range(len(flights)):
            if flights[index][0] == place:
                flight(index, which, kv).start()

    def arrived(place, which, kv):
        for index in range(len(flights)):
            if flights[index][1][2] == place:
                flight(index, which, kv).wait_recv()

    tiles = share // TILE
    n_half = tiles * group // 2

    def sweep(units, n_keys, lifted, done):
        chunks = n_keys // KB
        tops, sums = {}, {}

        def scores(i, c):
            b, load, at = units[i]
            piece = load(c)
            s = jnp.dot(
                jnp.concatenate([piece, piece], axis=1), q_t[b], preferred_element_type=jnp.float32
            )
            if lifted:
                pair = b % n_half // tiles
                wide = lax.broadcasted_iota(jnp.int32, (1, QB), 1)
                s = s + jnp.where(wide < TILE, lift[2 * pair], lift[2 * pair + 1]) * LOG2E
            s_buf[i % (AHEAD + 1), c * KB : (c + 1) * KB, :] = s
            high = jnp.max(s.reshape(KB // 8, 8, QB), axis=0)
            tops[i] = jnp.maximum(tops[i], high) if i in tops else high

        for i in range(AHEAD):
            for c in range(chunks):
                scores(i, c)
        for i, (b, load, at) in enumerate(units):
            m_old = m_st[b]
            m = jnp.maximum(m_old, jnp.max(tops.pop(i), axis=0, keepdims=True))
            m_st[b] = m
            alpha = jnp.exp2(m_old - m)
            o = None
            for c in range(chunks):
                if i + AHEAD < len(units):
                    scores(i + AHEAD, c)
                x = s_buf[i % (AHEAD + 1), c * KB : (c + 1) * KB, :].reshape(KB // 8, 8, QB) - m[None]
                p = jnp.exp2(x).reshape(KB, QB).astype(jnp.bfloat16)
                values = v_t[:, at + c * KB : at + (c + 1) * KB]
                term = jnp.dot(values, p, preferred_element_type=jnp.float32)
                o = term if o is None else o + term
            o = acc[b] * alpha[0:1] + o
            if done is None:
                acc[b] = o
            else:
                done(b, o)

    def group_sweep(step, order, which, kv):
        if which is not None:
            for k, places in enumerate(GROUPS):
                @pl.when(step == k)
                def _(k=k, places=places):
                    for place in places:
                        if place != (0, 0):
                            arrived(place, which, kv)
                            pass_on(place, which, kv)

        ids = [pick(step, [slot_of(places[i]) for places in GROUPS]) for i in range(4)]

        def tile_at(t):
            return kv[ids[t // tiles], t % tiles * TILE : (t % tiles + 1) * TILE, :]

        for t in range(4 * tiles):
            v_t[:HD, t * TILE : (t + 1) * TILE] = tile_at(t).T[HD:]
        per = KB // TILE

        def loader(base):
            return lambda c: jnp.concatenate([tile_at(base + c * per + i) for i in range(per)], axis=0)

        units = [(b, loader(2 * tiles * pair), 2 * share * pair) for pair in range(2) for b in order]
        sweep(units, 2 * share, False, None)

    v_t[HD:, :] = jnp.ones((v_t.shape[0] - HD, v_t.shape[1]), jnp.bfloat16)
    acc[...] = jnp.zeros_like(acc)
    m_st[...] = jnp.full(m_st.shape, -1e30, jnp.float32)

    first_half, second_half = list(range(n_half)), list(range(n_half, 2 * n_half))
    local[4].wait()
    local[5].wait()
    absorb_keys(latent[...], tp, 0, kv1, 0)
    lat[0].wait_recv()
    send_rows(4, raw.at[0, top], 2, top, right_tp)
    absorb_keys(raw[0, top, :], left_tp, 0, kv1, rows)
    lat[1].wait_recv()
    absorb_keys(raw[1, top, :], right_tp, 0, kv1, rows + half)
    pass_on((0, 0), 0, kv1)
    local[6].wait()
    absorb_queries([(tp, 0, rows), (left_tp, 0, half), (right_tp, 0, half)], 0)

    last_rows = send(raw.at[1, low], raw.at[2, low], lat_send.at[5], lat_recv.at[5], {"tp": left_tp})

    def one(step, carry):
        @pl.when(step == 1)
        def _():
            lat[3].wait_recv()
            last_rows.start()

        group_sweep(step, first_half, 0, kv1)
        return carry

    lax.fori_loop(0, len(GROUPS), one, 0)

    local[3].wait()
    x = key_value(modulated(context[...], 1))
    kv2[0, share : share + ctx_rows, :] = jnp.where(left, headed(x, kg), x).astype(jnp.bfloat16)
    lat[2].wait_recv()
    absorb_keys(raw[0, low, :], left_tp, half, kv2, 0)
    absorb_keys(raw[1, low, :], right_tp, half, kv2, half)
    lat[4].wait_recv()
    last_rows.wait_recv()
    absorb_keys(raw[2], far_tp, 0, kv2, rows)
    pass_on((0, 0), 1, kv2)
    absorb_queries([(left_tp, half, half), (right_tp, half, half), (far_tp, 0, rows)], n_half)

    def two(step, carry):
        group_sweep(step, second_half, None, kv1)
        return carry

    lax.fori_loop(0, len(GROUPS), two, 0)

    def three(step, carry):
        group_sweep(step, first_half + second_half, 1, kv2)
        return carry

    lax.fori_loop(0, len(GROUPS), three, 0)

    def done(b, o):
        o = (o[:HD] / o[HD : HD + 1]).astype(jnp.bfloat16).astype(jnp.float32)
        both = jnp.concatenate([o[:, :TILE], o[:, TILE:]], axis=0)
        pair, tile = b % n_half // tiles, b % n_half % tiles
        at = b // n_half * share + tile * TILE
        o_tok[at : at + TILE, pair * 2 * HD : (pair + 1) * 2 * HD] = both.T.astype(jnp.bfloat16)

    for slot in range(n_sp):
        kv_ctx[slot * ctx_rows : (slot + 1) * ctx_rows, :] = kv2[slot, share:, :]
    n_ctx = n_sp * ctx_rows
    for t in range(n_ctx // TILE):
        v_t[:HD, t * TILE : (t + 1) * TILE] = kv_ctx[t * TILE : (t + 1) * TILE, :].T[HD:]
    units = [(b, lambda c: kv_ctx[c * KB : (c + 1) * KB, :], 0) for b in second_half + first_half]
    sweep(units, n_ctx, True, done)

    span = group * HD
    mine = pl.ds(pl.multiple_of(tp * span, span), span)
    o_copies = []
    for i, (at, count, owner, start) in enumerate(
        (
            (share + rows, rows, far_tp, 0),
            (share, half, left_tp, half),
            (share + half, half, right_tp, half),
            (rows, half, left_tp, 0),
            (rows + half, half, right_tp, 0),
        )
    ):
        copy = send(
            o_tok.at[at : at + count], o_all.at[start : start + count, mine],
            o_ssem.at[i], o_rsem.at[i], {"tp": owner},
        )
        copy.start()
        o_copies.append(copy)
    o_all[:, mine] = o_tok[0:rows, :]
    local[7].wait()
    for copy in o_copies:
        copy.wait_recv()

    for j in range(n_tp):
        cols = pl.ds(j * chunk, chunk)
        y_j = jnp.dot(o_all[...], wout[:, cols], preferred_element_type=jnp.float32)
        gate = mods_all[j, 4:5, :]
        out[:, cols] = (latent[:, cols].astype(jnp.float32) + gate * y_j).astype(jnp.bfloat16)

    for copy in lat + [last_rows] + pa + pb + o_copies:
        copy.wait_send()
    for index in range(len(flights)):
        flight(index, 0, kv1).wait_send()
        flight(index, 1, kv2).wait_send()


def on_device(n_sp, n_tp, latent, cond, cond_ctx, context, norm_gain, mod_shift, mod_scale, mod_gate,
              w_query, w_key, w_value, q_gain, k_gain, ctx_lift, w_out):
    _, rows, width = latent.shape
    tokens = rows * n_tp
    ctx_rows = context.shape[1]
    group = w_query.shape[1] // w_key.shape[1]
    keys = tokens + ctx_rows
    row_tab, col_tab = rope_tables(tokens * n_sp // GRID_W)
    chunk = mod_shift.shape[1]
    share = tokens // 2
    n_q = tokens // TILE * group // 2
    bf, f32 = jnp.bfloat16, jnp.float32
    vmem = pl.BlockSpec(memory_space=pltpu.VMEM)
    smem = pl.BlockSpec(memory_space=pltpu.SMEM)
    hbm = pl.BlockSpec(memory_space=pl.ANY)
    dma = pltpu.SemaphoreType.DMA
    out = pl.pallas_call(
        functools.partial(kernel, n_sp, n_tp, group),
        out_shape=jax.ShapeDtypeStruct((rows, width), bf),
        in_specs=[vmem] * 6 + [smem] + [vmem] * 2 + [hbm] * 8,
        out_specs=vmem,
        scratch_shapes=[
            pltpu.VMEM((ctx_rows, width), bf),
            pltpu.VMEM((3,) + mod_shift.shape, bf),
            pltpu.VMEM(w_query.shape, bf),
            pltpu.VMEM((2 * HD, width), bf),
            pltpu.VMEM(w_out.shape, bf),
            pltpu.VMEM((n_tp - 1, rows, width), bf),
            pltpu.VMEM((8, chunk), f32),
            pltpu.VMEM((n_sp - 1, 8, chunk), f32),
            pltpu.VMEM((n_tp, 8, chunk), f32),
            pltpu.VMEM((8, width), f32),
            pltpu.VMEM((2, tokens, 2 * HD), f32),
            pltpu.VMEM((share, width), bf),
            pltpu.VMEM((n_q, 4 * HD, QB), bf),
            pltpu.VMEM((n_sp, share, 2 * HD), bf),
            pltpu.VMEM((n_sp, share + ctx_rows, 2 * HD), bf),
            pltpu.VMEM((n_sp * ctx_rows, 2 * HD), bf),
            pltpu.VMEM((HD + 16, 2 * tokens), bf),
            pltpu.VMEM((AHEAD + 1, tokens, QB), f32),
            pltpu.VMEM((n_q, HD + 16, QB), f32),
            pltpu.VMEM((n_q, 8, QB), f32),
            pltpu.VMEM((tokens, group * HD), bf),
            pltpu.VMEM((rows, n_tp * group * HD), bf),
            dma((8,)),
            dma((6,)), dma((6,)),
            dma((n_sp - 1,)), dma((n_sp - 1,)),
            dma((n_tp - 1,)), dma((n_tp - 1,)),
            dma((2, n_sp - 1)), dma((2, n_sp)),
            dma((5,)), dma((5,)),
        ],
        compiler_params=pltpu.CompilerParams(
            collective_id=0, has_side_effects=True, vmem_limit_bytes=60 * 1024 * 1024,
        ),
    )(
        latent[0], cond, cond_ctx[None], norm_gain.reshape(width // TILE, TILE), q_gain[None], k_gain[None], ctx_lift,
        jnp.asarray(row_tab), jnp.asarray(col_tab),
        context[0], mod_shift, mod_scale, mod_gate, w_query, w_key.T, w_value.T, w_out,
    )
    return out[None]


def solution(mesh):
    placed = (
        P("dp", ("sp", "tp"), None),
        P("dp", "sp"),
        P("sp"),
        P("dp", "sp", None),
        P(),
        P("sp", "tp"),
        P("sp", "tp"),
        P("sp", "tp"),
        P(None, "tp"),
        P(None, "tp"),
        P(None, "tp"),
        P(),
        P(),
        P("tp"),
        P(),
    )
    return jax.shard_map(
        functools.partial(on_device, mesh.shape["sp"], mesh.shape["tp"]),
        mesh=mesh,
        in_specs=placed,
        out_specs=P("dp", ("sp", "tp"), None),
        check_vma=False,
    )
```

```python
import functools

import jax
import jax.numpy as jnp
import numpy as np
from jax import lax
from jax.experimental import pallas as pl
from jax.experimental.pallas import tpu as pltpu
from jax.sharding import PartitionSpec as P

HD = 64
GRID_W = 128
EPS = 1e-06
THETA = 10000.0
MESH = pl.DeviceIdType.MESH
LOG2E = 1.4426950408889634
QB = 256
KB = 256
TILE = 128

PAIRS = (
    ((0, 0), (3, 0)), ((1, 0), (0, 3)), ((0, 1), (2, 0)), ((3, 3), (3, 1)),
    ((1, 3), (1, 1)), ((2, 1), (0, 2)), ((2, 3), (3, 2)), ((1, 2), (2, 2)),
)
GROUPS = (
    ((0, 0), (3, 0), (1, 0), (0, 3)),
    ((0, 1), (2, 0), (3, 3), (3, 1)),
    ((1, 3), (1, 1), (2, 3), (2, 1)),
    ((0, 2), (3, 2), (1, 2), (2, 2)),
)
AHEAD = 3
FIRST_EVENTS = {
    0: ((3, 0), (1, 0), (0, 3)), 2: ((2, 0), (3, 1), (0, 1)), 3: ((3, 3),), 4: ((1, 3), (1, 1)),
    5: ((2, 1), (0, 2)), 6: ((2, 3), (3, 2)), 7: ((1, 2), (2, 2)),
}
EARLY_EVENTS = {1: ((3, 0), (1, 0), (0, 3)), 3: ((2, 0), (3, 3), (3, 1), (0, 1))}
LATE_EVENTS = {0: ((1, 3), (1, 1)), 1: ((2, 3), (2, 1)), 2: ((0, 2), (3, 2)), 3: ((1, 2), (2, 2))}
ONWARD = {
    (0, 0): ((0, 1, (3, 0)), (0, -1, (1, 0)), (1, 1, (0, 3)), (1, -1, (0, 1))),
    (3, 0): ((0, 1, (2, 0)), (1, 1, (3, 3)), (1, -1, (3, 1))),
    (1, 0): ((1, 1, (1, 3)), (1, -1, (1, 1))),
    (2, 0): ((1, 1, (2, 3)), (1, -1, (2, 1))),
    (0, 3): ((1, 1, (0, 2)),),
    (1, 3): ((1, 1, (1, 2)),),
    (3, 1): ((1, -1, (3, 2)),),
    (2, 1): ((1, -1, (2, 2)),),
}


def slot_of(place):
    return place[0] * 4 + place[1]


def pick(step, values):
    chosen = values[0]
    for i, value in enumerate(values[1:], 1):
        chosen = jnp.where(step == i, value, chosen)
    return chosen


def rope_tables(grid_rows):
    n = HD // 4
    inverse = (np.float32(THETA) ** (-np.arange(n, dtype=np.float32) / np.float32(n))).astype(np.float32)

    def table(count, low):
        angles = (np.arange(count, dtype=np.float32)[:, None] * inverse).astype(np.float32)
        zero = np.zeros((count, 2 * n), np.float32)
        sign = np.tile(np.array([-1.0, 1.0], np.float32), n)
        c = np.repeat(np.cos(angles.astype(np.float64)), 2, axis=1).astype(np.float32)
        s = np.repeat(np.sin(angles.astype(np.float64)), 2, axis=1).astype(np.float32) * sign
        parts = ([c, zero], [s, zero]) if low else ([zero, c], [zero, s])
        return [np.tile(np.concatenate(p, axis=1), (1, 2)) for p in parts]

    return np.stack(table(grid_rows, True)), np.stack(table(GRID_W, False))


def kernel(
    n_sp, n_tp, group,
    latent, cond, cond_ctx, norm_gain, q_gain, k_gain, lift, row_tab, col_tab,
    context_h, mshift_h, mscale_h, mgate_h, wq_h, wk_h, wv_h, wout_h,
    out,
    context, mods_w, wq, wkv, wout,
    raw, part, part_in, mods_all, ab, rope, u_buf, q_t, kv1, kv2, kv_ctx, v_t, s_buf, acc, m_st, o_tok, o_all,
    local_sem, lat_send, lat_recv, pa_send, pa_recv, pb_send, pb_recv, kv_send, kv_recv, o_ssem, o_rsem,
):
    rows = latent.shape[0]
    half = rows // 2
    width = latent.shape[1]
    chunk = width // n_tp
    tokens = rows * n_tp
    share = tokens // 2
    ctx_rows = context.shape[0]
    sp = lax.axis_index("sp")
    tp = lax.axis_index("tp")
    dp = lax.axis_index("dp")
    left_tp, right_tp, far_tp = (tp + n_tp - 1) % n_tp, (tp + 1) % n_tp, (tp + 2) % n_tp
    peers = (left_tp, right_tp, far_tp)
    sp_order = sorted(range(1, n_sp), key=lambda d: min(d, n_sp - d))

    local = [
        pltpu.make_async_copy(src, dst, local_sem.at[i])
        for i, (src, dst) in enumerate(
            (
                (mshift_h, mods_w.at[0]),
                (mscale_h, mods_w.at[1]),
                (mgate_h, mods_w.at[2]),
                (context_h, context),
                (wk_h, wkv.at[0:HD]),
                (wv_h, wkv.at[HD : 2 * HD]),
                (wq_h, wq),
                (wout_h, wout),
            )
        )
    ]
    for copy in local:
        copy.start()

    barrier = pltpu.get_barrier_semaphore()
    for peer in peers:
        pl.semaphore_signal(barrier, inc=1, device_id={"tp": peer}, device_id_type=MESH)
    for d in range(1, n_sp):
        pl.semaphore_signal(barrier, inc=1, device_id={"sp": (sp + d) % n_sp}, device_id_type=MESH)
    pl.semaphore_wait(barrier, n_tp - 1 + n_sp - 1)

    def send(src, dst, ssem, rsem, device):
        return pltpu.make_async_remote_copy(
            src_ref=src, dst_ref=dst, send_sem=ssem, recv_sem=rsem, device_id=device, device_id_type=MESH
        )

    top, low = pl.ds(0, half), pl.ds(half, half)
    lat = []

    def send_rows(index, src, slot, piece, peer):
        copy = send(src, raw.at[slot, piece], lat_send.at[index], lat_recv.at[index], {"tp": peer})
        copy.start()
        lat.append(copy)

    send_rows(0, latent.at[top], 0, top, right_tp)
    send_rows(1, latent.at[top], 1, top, left_tp)

    act = jnp.concatenate([cond[...], cond_ctx[...]], axis=0).astype(jnp.float32)
    act = (act / (1.0 + jnp.exp(-act))).astype(jnp.bfloat16)
    act = jnp.concatenate([act, jnp.zeros((14, act.shape[1]), jnp.bfloat16)], axis=0)
    for i in range(3):
        local[i].wait()
    sums = [jnp.dot(act, mods_w[i], preferred_element_type=jnp.float32)[0:2] for i in range(3)]
    part[...] = jnp.concatenate(sums + [jnp.zeros((2, chunk), jnp.float32)], axis=0)
    pa = []
    for d in sp_order:
        copy = send(part, part_in.at[d - 1], pa_send.at[d - 1], pa_recv.at[d - 1], {"sp": (sp + d) % n_sp})
        copy.start()
        pa.append(copy)

    groups = tokens // GRID_W
    for i in range(2):
        for g in range(groups):
            rope[i, pl.ds(g * GRID_W, GRID_W), :] = (
                row_tab[i, pl.ds(sp * groups + g, 1), :] + col_tab[i, :, :]
            )

    total = part[...]
    for copy in pa:
        copy.wait_recv()
    for d in range(1, n_sp):
        total = total + part_in[d - 1]
    mods_all[tp] = total
    pb = []
    for i, peer in enumerate((far_tp, left_tp, right_tp)):
        copy = send(mods_all.at[tp], mods_all.at[tp], pb_send.at[i], pb_recv.at[i], {"tp": peer})
        copy.start()
        pb.append(copy)
    send_rows(2, latent.at[low], 0, low, right_tp)
    send_rows(3, latent.at[low], 1, low, left_tp)

    for i, peer in enumerate((far_tp, left_tp, right_tp)):
        pb[i].wait_recv()
    for j in range(n_tp):
        block = mods_all[j]
        for i in range(chunk // TILE):
            at = j * chunk + i * TILE
            gain = norm_gain[at // TILE : at // TILE + 1, :].astype(jnp.float32)
            ab[0:2, at : at + TILE] = gain * (1.0 + block[2:4, i * TILE : (i + 1) * TILE])
        ab[2:4, pl.ds(j * chunk, chunk)] = block[0:2]

    lane = lax.broadcasted_iota(jnp.int32, (1, 2 * HD), 1)
    even = lane % 2 == 0
    left = lane < HD
    ones = (
        (lax.broadcasted_iota(jnp.int32, (2 * HD, 2 * HD), 0) < HD)
        == (lax.broadcasted_iota(jnp.int32, (2 * HD, 2 * HD), 1) < HD)
    ).astype(jnp.bfloat16)
    qg = jnp.concatenate([q_gain[...]] * 2, axis=1).astype(jnp.float32)
    kg = jnp.concatenate([k_gain[...]] * 2, axis=1).astype(jnp.float32)
    factor = LOG2E * HD ** (-0.5)

    def modulated(block, row):
        values = block.astype(jnp.float32)
        scale = lax.rsqrt(jnp.mean(values * values, axis=-1, keepdims=True) + EPS)
        return (values * scale * ab[row : row + 1, :] + ab[row + 2 : row + 3, :]).astype(jnp.bfloat16)

    def headed(x, g):
        square = x * x
        high = square.astype(jnp.bfloat16)
        rest = (square - high.astype(jnp.float32)).astype(jnp.bfloat16)
        mean = (
            jnp.dot(high, ones, preferred_element_type=jnp.float32)
            + jnp.dot(rest, ones, preferred_element_type=jnp.float32)
        ) * (1.0 / HD)
        return x * lax.rsqrt(mean + EPS) * g

    def turned(x, cosine, sine):
        partner = jnp.where(even, pltpu.roll(x, 2 * HD - 1, 1), pltpu.roll(x, 1, 1))
        return x * cosine + partner * sine

    def key_value(u):
        return lax.dot_general(u, wkv[...], (((1,), (1,)), ((), ())), preferred_element_type=jnp.float32)

    def angles(owner, start, count):
        where = pl.ds(pl.multiple_of(owner * rows + start, half), count)
        return rope[0, where, :], rope[1, where, :]

    def tables_of(pieces):
        tables = [angles(*piece) for piece in pieces]
        return [jnp.concatenate([t[i] for t in tables], axis=0) for i in range(2)]

    def absorb_keys(block, pieces, kv):
        u = modulated(block, 0)
        u_buf[...] = u
        cosine, sine = tables_of(pieces)
        x = key_value(u)
        kv[0, :share, :] = jnp.where(left, turned(headed(x, kg), cosine, sine), x).astype(jnp.bfloat16)

    def absorb_queries(pieces, first):
        cosine, sine = tables_of(pieces)
        raw_q = jnp.dot(u_buf[...], wq[...], preferred_element_type=jnp.float32)
        none = jnp.zeros((HD, QB), jnp.bfloat16)
        for pair in range(group // 2):
            x = raw_q[:, pair * 2 * HD : (pair + 1) * 2 * HD]
            x = turned(headed(x, qg), cosine, sine).astype(jnp.bfloat16).astype(jnp.float32) * factor
            for tile in range(tiles):
                t = x[tile * TILE : (tile + 1) * TILE, :].T
                t = jnp.concatenate([t[:HD], t[HD:]], axis=1)
                high = t.astype(jnp.bfloat16)
                rest = (t - high.astype(jnp.float32)).astype(jnp.bfloat16)
                q_t[first + pair * tiles + tile] = jnp.concatenate([high, none, rest, none], axis=0)

    side = int(round(n_sp ** 0.5))
    y, z = sp % side, sp // side

    def neighbour(axis, step):
        along_y = z * side + (y + step + side) % side
        along_z = (z + step + side) % side * side + y
        return jnp.where(dp == axis, along_y, along_z)

    flights = [(place, hop) for place in ONWARD for hop in ONWARD[place]]

    def flight(index, which, kv):
        place, (axis, step, target) = flights[index]
        return send(
            kv.at[slot_of(place)], kv.at[slot_of(target)],
            kv_send.at[which, index], kv_recv.at[which, slot_of(target)],
            {"sp": neighbour(axis, step)},
        )

    def pass_on(place, which, kv):
        for index in range(len(flights)):
            if flights[index][0] == place:
                flight(index, which, kv).start()

    def arrived(place, which, kv):
        for index in range(len(flights)):
            if flights[index][1][2] == place:
                flight(index, which, kv).wait_recv()

    tiles = share // TILE
    n_half = tiles * group // 2

    def sweep(units, n_keys, lifted, done):
        chunks = n_keys // KB
        tops, sums = {}, {}

        def scores(i, c):
            b, load, at = units[i]
            piece = load(c)
            s = jnp.dot(
                jnp.concatenate([piece, piece], axis=1), q_t[b], preferred_element_type=jnp.float32
            )
            if lifted:
                pair = b % n_half // tiles
                wide = lax.broadcasted_iota(jnp.int32, (1, QB), 1)
                s = s + jnp.where(wide < TILE, lift[2 * pair], lift[2 * pair + 1]) * LOG2E
            s_buf[i % (AHEAD + 1), c * KB : (c + 1) * KB, :] = s
            high = jnp.max(s.reshape(KB // 8, 8, QB), axis=0)
            tops[i] = jnp.maximum(tops[i], high) if i in tops else high

        for i in range(AHEAD):
            for c in range(chunks):
                scores(i, c)
        for i, (b, load, at) in enumerate(units):
            m_old = m_st[b]
            m = jnp.maximum(m_old, jnp.max(tops.pop(i), axis=0, keepdims=True))
            m_st[b] = m
            alpha = jnp.exp2(m_old - m)
            o = None
            for c in range(chunks):
                if i + AHEAD < len(units):
                    scores(i + AHEAD, c)
                x = s_buf[i % (AHEAD + 1), c * KB : (c + 1) * KB, :].reshape(KB // 8, 8, QB) - m[None]
                p = jnp.exp2(x).reshape(KB, QB).astype(jnp.bfloat16)
                values = v_t[:, at + c * KB : at + (c + 1) * KB]
                term = jnp.dot(values, p, preferred_element_type=jnp.float32)
                o = term if o is None else o + term
            o = acc[b] * alpha[0:1] + o
            if done is None:
                acc[b] = o
            else:
                done(b, o)

    def group_sweep(step, order, table, kv, events, which, moved):
        for k in events:
            @pl.when(step == k)
            def _(k=k):
                for place in events[k]:
                    arrived(place, which, moved)
                    pass_on(place, which, moved)

        many = len(table[0])
        ids = [pick(step, [slot_of(places[i]) for places in table]) for i in range(many)]

        def tile_at(t):
            return kv[ids[t // tiles], t % tiles * TILE : (t % tiles + 1) * TILE, :]

        for t in range(many * tiles):
            v_t[:HD, t * TILE : (t + 1) * TILE] = tile_at(t).T[HD:]
        per = KB // TILE

        def loader(base):
            return lambda c: jnp.concatenate([tile_at(base + c * per + i) for i in range(per)], axis=0)

        units = [(b, loader(2 * tiles * pair), 2 * share * pair) for pair in range(many // 2) for b in order]
        sweep(units, 2 * share, False, None)

    v_t[HD:, :] = jnp.ones((v_t.shape[0] - HD, v_t.shape[1]), jnp.bfloat16)
    acc[...] = jnp.zeros_like(acc)
    m_st[...] = jnp.full(m_st.shape, -1e30, jnp.float32)

    first_half, second_half = list(range(n_half)), list(range(n_half, 2 * n_half))
    local[4].wait()
    local[5].wait()
    near = [(tp, 0, rows), (left_tp, 0, half), (right_tp, 0, half)]
    lat[0].wait_recv()
    send_rows(4, raw.at[0, top], 2, top, right_tp)
    lat[1].wait_recv()
    absorb_keys(jnp.concatenate([latent[...], raw[0, top, :], raw[1, top, :]], axis=0), near, kv1)
    pass_on((0, 0), 0, kv1)
    local[6].wait()
    absorb_queries(near, 0)
    local[3].wait()
    x = key_value(modulated(context[...], 1))
    kv2[0, share : share + ctx_rows, :] = jnp.where(left, headed(x, kg), x).astype(jnp.bfloat16)

    last_rows = send(raw.at[1, low], raw.at[2, low], lat_send.at[5], lat_recv.at[5], {"tp": left_tp})

    def one(step, carry):
        @pl.when(step == 3)
        def _():
            lat[3].wait_recv()
            last_rows.start()

        group_sweep(step, first_half, PAIRS, kv1, FIRST_EVENTS, 0, kv1)
        return carry

    lax.fori_loop(0, len(PAIRS), one, 0)

    far = [(left_tp, half, half), (right_tp, half, half), (far_tp, 0, rows)]
    lat[2].wait_recv()
    lat[4].wait_recv()
    last_rows.wait_recv()
    absorb_keys(jnp.concatenate([raw[0, low, :], raw[1, low, :], raw[2]], axis=0), far, kv2)
    pass_on((0, 0), 1, kv2)
    absorb_queries(far, n_half)

    def two(step, carry):
        group_sweep(step, second_half, GROUPS, kv1, EARLY_EVENTS, 1, kv2)
        return carry

    lax.fori_loop(0, len(GROUPS), two, 0)

    def three(step, carry):
        group_sweep(step, second_half, GROUPS, kv2, LATE_EVENTS, 1, kv2)
        return carry

    lax.fori_loop(0, len(GROUPS), three, 0)

    def done(b, o):
        o = (o[:HD] / o[HD : HD + 1]).astype(jnp.bfloat16).astype(jnp.float32)
        both = jnp.concatenate([o[:, :TILE], o[:, TILE:]], axis=0)
        pair, tile = b % n_half // tiles, b % n_half % tiles
        at = b // n_half * share + tile * TILE
        o_tok[at : at + TILE, pair * 2 * HD : (pair + 1) * 2 * HD] = both.T.astype(jnp.bfloat16)

    for slot in range(n_sp):
        kv_ctx[slot * ctx_rows : (slot + 1) * ctx_rows, :] = kv2[slot, share:, :]
    n_ctx = n_sp * ctx_rows
    span = group * HD
    mine = pl.ds(pl.multiple_of(tp * span, span), span)
    o_copies = []

    def finish(order):
        for t in range(n_ctx // TILE):
            v_t[:HD, t * TILE : (t + 1) * TILE] = kv_ctx[t * TILE : (t + 1) * TILE, :].T[HD:]
        units = [(b, lambda c: kv_ctx[c * KB : (c + 1) * KB, :], 0) for b in order]
        sweep(units, n_ctx, True, done)

    def send_back(at, count, owner, start):
        i = len(o_copies)
        copy = send(
            o_tok.at[at : at + count], o_all.at[start : start + count, mine],
            o_ssem.at[i], o_rsem.at[i], {"tp": owner},
        )
        copy.start()
        o_copies.append(copy)

    finish(second_half)
    send_back(share + rows, rows, far_tp, 0)
    send_back(share, half, left_tp, half)
    send_back(share + half, half, right_tp, half)

    def four(step, carry):
        group_sweep(step, first_half, GROUPS, kv2, {}, 1, kv2)
        return carry

    lax.fori_loop(0, len(GROUPS), four, 0)
    finish(first_half)
    send_back(rows, half, left_tp, 0)
    send_back(rows + half, half, right_tp, 0)
    o_all[:, mine] = o_tok[0:rows, :]
    local[7].wait()

    def output(where):
        for j in range(n_tp):
            cols = pl.ds(j * chunk, chunk)
            y_j = jnp.dot(o_all[where, :], wout[:, cols], preferred_element_type=jnp.float32)
            gate = mods_all[j, 4:5, :]
            out[where, cols] = (latent[where, cols].astype(jnp.float32) + gate * y_j).astype(jnp.bfloat16)

    for copy in o_copies[:3]:
        copy.wait_recv()
    output(low)
    for copy in o_copies[3:]:
        copy.wait_recv()
    output(top)

    for copy in lat + [last_rows] + pa + pb + o_copies:
        copy.wait_send()
    for index in range(len(flights)):
        flight(index, 0, kv1).wait_send()
        flight(index, 1, kv2).wait_send()


def on_device(n_sp, n_tp, latent, cond, cond_ctx, context, norm_gain, mod_shift, mod_scale, mod_gate,
              w_query, w_key, w_value, q_gain, k_gain, ctx_lift, w_out):
    _, rows, width = latent.shape
    tokens = rows * n_tp
    ctx_rows = context.shape[1]
    group = w_query.shape[1] // w_key.shape[1]
    keys = tokens + ctx_rows
    row_tab, col_tab = rope_tables(tokens * n_sp // GRID_W)
    chunk = mod_shift.shape[1]
    share = tokens // 2
    n_q = tokens // TILE * group // 2
    bf, f32 = jnp.bfloat16, jnp.float32
    vmem = pl.BlockSpec(memory_space=pltpu.VMEM)
    smem = pl.BlockSpec(memory_space=pltpu.SMEM)
    hbm = pl.BlockSpec(memory_space=pl.ANY)
    dma = pltpu.SemaphoreType.DMA
    out = pl.pallas_call(
        functools.partial(kernel, n_sp, n_tp, group),
        out_shape=jax.ShapeDtypeStruct((rows, width), bf),
        in_specs=[vmem] * 6 + [smem] + [vmem] * 2 + [hbm] * 8,
        out_specs=vmem,
        scratch_shapes=[
            pltpu.VMEM((ctx_rows, width), bf),
            pltpu.VMEM((3,) + mod_shift.shape, bf),
            pltpu.VMEM(w_query.shape, bf),
            pltpu.VMEM((2 * HD, width), bf),
            pltpu.VMEM(w_out.shape, bf),
            pltpu.VMEM((n_tp - 1, rows, width), bf),
            pltpu.VMEM((8, chunk), f32),
            pltpu.VMEM((n_sp - 1, 8, chunk), f32),
            pltpu.VMEM((n_tp, 8, chunk), f32),
            pltpu.VMEM((8, width), f32),
            pltpu.VMEM((2, tokens, 2 * HD), f32),
            pltpu.VMEM((share, width), bf),
            pltpu.VMEM((n_q, 4 * HD, QB), bf),
            pltpu.VMEM((n_sp, share, 2 * HD), bf),
            pltpu.VMEM((n_sp, share + ctx_rows, 2 * HD), bf),
            pltpu.VMEM((n_sp * ctx_rows, 2 * HD), bf),
            pltpu.VMEM((HD + 16, 2 * tokens), bf),
            pltpu.VMEM((AHEAD + 1, tokens, QB), f32),
            pltpu.VMEM((n_q, HD + 16, QB), f32),
            pltpu.VMEM((n_q, 8, QB), f32),
            pltpu.VMEM((tokens, group * HD), bf),
            pltpu.VMEM((rows, n_tp * group * HD), bf),
            dma((8,)),
            dma((6,)), dma((6,)),
            dma((n_sp - 1,)), dma((n_sp - 1,)),
            dma((n_tp - 1,)), dma((n_tp - 1,)),
            dma((2, n_sp - 1)), dma((2, n_sp)),
            dma((5,)), dma((5,)),
        ],
        compiler_params=pltpu.CompilerParams(
            collective_id=0, has_side_effects=True, vmem_limit_bytes=60 * 1024 * 1024,
        ),
    )(
        latent[0], cond, cond_ctx[None], norm_gain.reshape(width // TILE, TILE), q_gain[None], k_gain[None], ctx_lift,
        jnp.asarray(row_tab), jnp.asarray(col_tab),
        context[0], mod_shift, mod_scale, mod_gate, w_query, w_key.T, w_value.T, w_out,
    )
    return out[None]


def solution(mesh):
    placed = (
        P("dp", ("sp", "tp"), None),
        P("dp", "sp"),
        P("sp"),
        P("dp", "sp", None),
        P(),
        P("sp", "tp"),
        P("sp", "tp"),
        P("sp", "tp"),
        P(None, "tp"),
        P(None, "tp"),
        P(None, "tp"),
        P(),
        P(),
        P("tp"),
        P(),
    )
    return jax.shard_map(
        functools.partial(on_device, mesh.shape["sp"], mesh.shape["tp"]),
        mesh=mesh,
        in_specs=placed,
        out_specs=P("dp", ("sp", "tp"), None),
        check_vma=False,
    )
```

```python
import functools

import jax
import jax.numpy as jnp
import numpy as np
from jax import lax
from jax.experimental import pallas as pl
from jax.experimental.pallas import tpu as pltpu
from jax.sharding import PartitionSpec as P

HD = 64
GRID_W = 128
EPS = 1e-06
THETA = 10000.0
MESH = pl.DeviceIdType.MESH
LOG2E = 1.4426950408889634
QB = 256
KB = 256
TILE = 128

PAIRS = (
    ((0, 0), (3, 0)), ((1, 0), (0, 3)), ((0, 1), (2, 0)), ((3, 3), (3, 1)),
    ((1, 3), (1, 1)), ((2, 1), (0, 2)), ((2, 3), (3, 2)), ((1, 2), (2, 2)),
)
GROUPS = (
    ((0, 0), (3, 0), (1, 0), (0, 3)),
    ((0, 1), (2, 0), (3, 3), (3, 1)),
    ((1, 3), (1, 1), (2, 3), (2, 1)),
    ((0, 2), (3, 2), (1, 2), (2, 2)),
)
AHEAD = 3
ONWARD = {
    (0, 0): ((0, 1, (3, 0)), (0, -1, (1, 0)), (1, 1, (0, 3)), (1, -1, (0, 1))),
    (3, 0): ((0, 1, (2, 0)), (1, 1, (3, 3)), (1, -1, (3, 1))),
    (1, 0): ((1, 1, (1, 3)), (1, -1, (1, 1))),
    (2, 0): ((1, 1, (2, 3)), (1, -1, (2, 1))),
    (0, 3): ((1, 1, (0, 2)),),
    (1, 3): ((1, 1, (1, 2)),),
    (3, 1): ((1, -1, (3, 2)),),
    (2, 1): ((1, -1, (2, 2)),),
}


def slot_of(place):
    return place[0] * 4 + place[1]


def slots(groups, base):
    return [[base + slot_of(place) for place in places] for places in groups]


FIRST_EVENTS = {
    0: ((0, (3, 0)), (0, (1, 0)), (0, (0, 3))), 2: ((0, (2, 0)), (0, (3, 1)), (0, (0, 1))), 3: ((0, (3, 3)),),
    4: ((0, (1, 3)), (0, (1, 1))), 5: ((0, (2, 1)), (0, (0, 2))),
}
EARLY_EVENTS = {
    1: ((1, (3, 0)), (1, (1, 0)), (1, (0, 3))), 2: ((0, (2, 3)),),
    3: ((1, (2, 0)), (1, (3, 3)), (1, (3, 1)), (1, (0, 1)), (0, (3, 2)), (0, (1, 2)), (0, (2, 2))),
}
LATE_EVENTS = {
    0: ((1, (1, 3)), (1, (1, 1))), 1: ((1, (2, 3)), (1, (2, 1))), 2: ((1, (0, 2)), (1, (3, 2))),
    3: ((1, (1, 2)), (1, (2, 2))),
}


def pick(step, values):
    chosen = values[0]
    for i, value in enumerate(values[1:], 1):
        chosen = jnp.where(step == i, value, chosen)
    return chosen


def rope_tables(grid_rows):
    n = HD // 4
    inverse = (np.float32(THETA) ** (-np.arange(n, dtype=np.float32) / np.float32(n))).astype(np.float32)

    def table(count, low):
        angles = (np.arange(count, dtype=np.float32)[:, None] * inverse).astype(np.float32)
        zero = np.zeros((count, 2 * n), np.float32)
        sign = np.tile(np.array([-1.0, 1.0], np.float32), n)
        c = np.repeat(np.cos(angles.astype(np.float64)), 2, axis=1).astype(np.float32)
        s = np.repeat(np.sin(angles.astype(np.float64)), 2, axis=1).astype(np.float32) * sign
        parts = ([c, zero], [s, zero]) if low else ([zero, c], [zero, s])
        return [np.tile(np.concatenate(p, axis=1), (1, 2)) for p in parts]

    return np.stack(table(grid_rows, True)), np.stack(table(GRID_W, False))


def kernel(
    n_sp, n_tp, group,
    latent, cond, cond_ctx, norm_gain, q_gain, k_gain, lift, row_tab, col_tab,
    context_h, mshift_h, mscale_h, mgate_h, wq_h, wk_h, wv_h, wout_h,
    out,
    context, mods_w, wq, wkv, wout,
    raw, part, part_in, later, later_in, mods_all, mods_later, ab, rope, u_buf, q_t, kv, kv_ctx, v_t, s_buf, acc, m_st, o_tok, o_all,
    local_sem, lat_send, lat_recv, pa_send, pa_recv, pb_send, pb_recv, pc_send, pc_recv, pd_send, pd_recv, kv_send, kv_recv, o_ssem, o_rsem,
):
    rows = latent.shape[0]
    half = rows // 2
    width = latent.shape[1]
    chunk = width // n_tp
    tokens = rows * n_tp
    share = tokens // 2
    ctx_rows = context.shape[0]
    sp = lax.axis_index("sp")
    tp = lax.axis_index("tp")
    dp = lax.axis_index("dp")
    left_tp, right_tp, far_tp = (tp + n_tp - 1) % n_tp, (tp + 1) % n_tp, (tp + 2) % n_tp
    peers = (left_tp, right_tp, far_tp)
    sp_order = sorted(range(1, n_sp), key=lambda d: min(d, n_sp - d))

    local = [
        pltpu.make_async_copy(src, dst, local_sem.at[i])
        for i, (src, dst) in enumerate(
            (
                (mshift_h, mods_w.at[0]),
                (mscale_h, mods_w.at[1]),
                (mgate_h, mods_w.at[2]),
                (context_h, context),
                (wk_h, wkv.at[0:HD]),
                (wv_h, wkv.at[HD : 2 * HD]),
                (wq_h, wq),
                (wout_h, wout),
            )
        )
    ]
    for copy in local:
        copy.start()

    barrier = pltpu.get_barrier_semaphore()
    for peer in peers:
        pl.semaphore_signal(barrier, inc=1, device_id={"tp": peer}, device_id_type=MESH)
    for d in range(1, n_sp):
        pl.semaphore_signal(barrier, inc=1, device_id={"sp": (sp + d) % n_sp}, device_id_type=MESH)
    pl.semaphore_wait(barrier, n_tp - 1 + n_sp - 1)

    def send(src, dst, ssem, rsem, device):
        return pltpu.make_async_remote_copy(
            src_ref=src, dst_ref=dst, send_sem=ssem, recv_sem=rsem, device_id=device, device_id_type=MESH
        )

    top, low = pl.ds(0, half), pl.ds(half, half)
    lat = []

    def send_rows(index, src, slot, piece, peer):
        copy = send(src, raw.at[slot, piece], lat_send.at[index], lat_recv.at[index], {"tp": peer})
        copy.start()
        lat.append(copy)

    send_rows(0, latent.at[top], 0, top, right_tp)
    send_rows(1, latent.at[low], 1, low, left_tp)

    act = jnp.concatenate([cond[...], cond_ctx[...]], axis=0).astype(jnp.float32)
    act = (act / (1.0 + jnp.exp(-act))).astype(jnp.bfloat16)
    act = jnp.concatenate([act, jnp.zeros((14, act.shape[1]), jnp.bfloat16)], axis=0)
    for i in range(3):
        local[i].wait()
    sums = [jnp.dot(act, mods_w[i], preferred_element_type=jnp.float32)[0:2] for i in range(3)]
    per_chunk = chunk // TILE

    def stacked(rows_of):
        return jnp.concatenate(
            [r[:, i * TILE : (i + 1) * TILE] for r in rows_of for i in range(per_chunk)], axis=0
        )

    part[...] = stacked([sums[0][0:1], sums[1][0:1]])
    later[...] = stacked([sums[0][1:2], sums[1][1:2], sums[2][0:1], jnp.zeros((1, chunk), jnp.float32)])
    pa, pc = [], []
    for out_list, src, dst, ssem, rsem in (
        (pa, part, part_in, pa_send, pa_recv), (pc, later, later_in, pc_send, pc_recv)
    ):
        for d in sp_order:
            copy = send(src, dst.at[d - 1], ssem.at[d - 1], rsem.at[d - 1], {"sp": (sp + d) % n_sp})
            copy.start()
            out_list.append(copy)

    groups = tokens // GRID_W
    for i in range(2):
        for g in range(groups):
            rope[i, pl.ds(g * GRID_W, GRID_W), :] = (
                row_tab[i, pl.ds(sp * groups + g, 1), :] + col_tab[i, :, :]
            )

    total = part[...]
    for copy in pa:
        copy.wait_recv()
    for d in range(1, n_sp):
        total = total + part_in[d - 1]
    mods_all[tp] = total
    pb = []
    for i, peer in enumerate((far_tp, left_tp, right_tp)):
        copy = send(mods_all.at[tp], mods_all.at[tp], pb_send.at[i], pb_recv.at[i], {"tp": peer})
        copy.start()
        pb.append(copy)
    send_rows(2, latent.at[low], 0, low, right_tp)
    send_rows(3, latent.at[top], 1, top, left_tp)

    for copy in pb:
        copy.wait_recv()

    def set_ab(row, table):
        for j in range(n_tp):
            block = table[j]
            for i in range(per_chunk):
                at = j * chunk + i * TILE
                gain = norm_gain[at // TILE : at // TILE + 1, :].astype(jnp.float32)
                ab[row : row + 1, at : at + TILE] = gain * (1.0 + block[per_chunk + i : per_chunk + i + 1])
                ab[row + 2 : row + 3, at : at + TILE] = block[i : i + 1]

    set_ab(0, mods_all)

    lane = lax.broadcasted_iota(jnp.int32, (1, 2 * HD), 1)
    even = lane % 2 == 0
    left = lane < HD
    ones = (
        (lax.broadcasted_iota(jnp.int32, (2 * HD, 2 * HD), 0) < HD)
        == (lax.broadcasted_iota(jnp.int32, (2 * HD, 2 * HD), 1) < HD)
    ).astype(jnp.bfloat16)
    qg = jnp.concatenate([q_gain[...]] * 2, axis=1).astype(jnp.float32)
    kg = jnp.concatenate([k_gain[...]] * 2, axis=1).astype(jnp.float32)
    factor = LOG2E * HD ** (-0.5)

    def modulated(block, row):
        values = block.astype(jnp.float32)
        scale = lax.rsqrt(jnp.mean(values * values, axis=-1, keepdims=True) + EPS)
        return (values * scale * ab[row : row + 1, :] + ab[row + 2 : row + 3, :]).astype(jnp.bfloat16)

    def headed(x, g):
        square = x * x
        high = square.astype(jnp.bfloat16)
        rest = (square - high.astype(jnp.float32)).astype(jnp.bfloat16)
        mean = (
            jnp.dot(high, ones, preferred_element_type=jnp.float32)
            + jnp.dot(rest, ones, preferred_element_type=jnp.float32)
        ) * (1.0 / HD)
        return x * lax.rsqrt(mean + EPS) * g

    def turned(x, cosine, sine):
        partner = jnp.where(even, pltpu.roll(x, 2 * HD - 1, 1), pltpu.roll(x, 1, 1))
        return x * cosine + partner * sine

    def key_value(u):
        return lax.dot_general(u, wkv[...], (((1,), (1,)), ((), ())), preferred_element_type=jnp.float32)

    def angles(owner, start, count):
        where = pl.ds(pl.multiple_of(owner * rows + start, half), count)
        return rope[0, where, :], rope[1, where, :]

    def tables_of(pieces):
        tables = [angles(*piece) for piece in pieces]
        return [jnp.concatenate([t[i] for t in tables], axis=0) for i in range(2)]

    def absorb_keys(block, pieces, slot):
        u = modulated(block, 0)
        u_buf[...] = u
        cosine, sine = tables_of(pieces)
        x = key_value(u)
        kv[slot, :share, :] = jnp.where(left, turned(headed(x, kg), cosine, sine), x).astype(jnp.bfloat16)

    def absorb_queries(pieces, first):
        cosine, sine = tables_of(pieces)
        raw_q = jnp.dot(u_buf[...], wq[...], preferred_element_type=jnp.float32)
        none = jnp.zeros((HD, QB), jnp.bfloat16)
        for pair in range(group // 2):
            x = raw_q[:, pair * 2 * HD : (pair + 1) * 2 * HD]
            x = turned(headed(x, qg), cosine, sine).astype(jnp.bfloat16).astype(jnp.float32) * factor
            for tile in range(tiles):
                t = x[tile * TILE : (tile + 1) * TILE, :].T
                t = jnp.concatenate([t[:HD], t[HD:]], axis=1)
                high = t.astype(jnp.bfloat16)
                rest = (t - high.astype(jnp.float32)).astype(jnp.bfloat16)
                q_t[first + pair * tiles + tile] = jnp.concatenate([high, none, rest, none], axis=0)

    side = int(round(n_sp ** 0.5))
    y, z = sp % side, sp // side

    def neighbour(axis, step):
        along_y = z * side + (y + step + side) % side
        along_z = (z + step + side) % side * side + y
        return jnp.where(dp == axis, along_y, along_z)

    flights = [(place, hop) for place in ONWARD for hop in ONWARD[place]]

    def flight(index, which):
        place, (axis, step, target) = flights[index]
        piece = pl.ds(0, share + which * ctx_rows)
        base = which * n_sp
        return send(
            kv.at[base + slot_of(place), piece], kv.at[base + slot_of(target), piece],
            kv_send.at[which, index], kv_recv.at[which, slot_of(target)],
            {"sp": neighbour(axis, step)},
        )

    def pass_on(place, which):
        for index in range(len(flights)):
            if flights[index][0] == place:
                flight(index, which).start()

    def arrived(place, which):
        for index in range(len(flights)):
            if flights[index][1][2] == place:
                flight(index, which).wait_recv()

    tiles = share // TILE
    n_half = tiles * group // 2

    def sweep(units, n_keys, lifted, done):
        chunks = n_keys // KB
        tops, sums = {}, {}

        def scores(i, c):
            b, load, at = units[i]
            piece = load(c)
            s = jnp.dot(
                jnp.concatenate([piece, piece], axis=1), q_t[b], preferred_element_type=jnp.float32
            )
            if lifted:
                pair = b % n_half // tiles
                wide = lax.broadcasted_iota(jnp.int32, (1, QB), 1)
                s = s + jnp.where(wide < TILE, lift[2 * pair], lift[2 * pair + 1]) * LOG2E
            s_buf[i % (AHEAD + 1), c * KB : (c + 1) * KB, :] = s
            high = jnp.max(s.reshape(KB // 8, 8, QB), axis=0)
            tops[i] = jnp.maximum(tops[i], high) if i in tops else high

        for i in range(AHEAD):
            for c in range(chunks):
                scores(i, c)
        for i, (b, load, at) in enumerate(units):
            m_old = m_st[b]
            m = jnp.maximum(m_old, jnp.max(tops.pop(i), axis=0, keepdims=True))
            m_st[b] = m
            alpha = jnp.exp2(m_old - m)
            o = None
            for c in range(chunks):
                if i + AHEAD < len(units):
                    scores(i + AHEAD, c)
                x = s_buf[i % (AHEAD + 1), c * KB : (c + 1) * KB, :].reshape(KB // 8, 8, QB) - m[None]
                p = jnp.exp2(x).reshape(KB, QB).astype(jnp.bfloat16)
                values = v_t[:, at + c * KB : at + (c + 1) * KB]
                term = jnp.dot(values, p, preferred_element_type=jnp.float32)
                o = term if o is None else o + term
            o = acc[b] * alpha[0:1] + o
            if done is None:
                acc[b] = o
            else:
                done(b, o)

    def group_sweep(step, order, table, events):
        for k in events:
            @pl.when(step == k)
            def _(k=k):
                for which, place in events[k]:
                    arrived(place, which)
                    pass_on(place, which)

        many = len(table[0])
        ids = [pick(step, [places[i] for places in table]) for i in range(many)]

        def tile_at(t):
            return kv[ids[t // tiles], t % tiles * TILE : (t % tiles + 1) * TILE, :]

        for t in range(many * tiles):
            v_t[:HD, t * TILE : (t + 1) * TILE] = tile_at(t).T[HD:]
        per = KB // TILE

        def loader(base):
            return lambda c: jnp.concatenate([tile_at(base + c * per + i) for i in range(per)], axis=0)

        units = [(b, loader(2 * tiles * pair), 2 * share * pair) for pair in range(many // 2) for b in order]
        sweep(units, 2 * share, False, None)

    v_t[HD:, :] = jnp.ones((v_t.shape[0] - HD, v_t.shape[1]), jnp.bfloat16)
    acc[...] = jnp.zeros_like(acc)
    m_st[...] = jnp.full(m_st.shape, -1e30, jnp.float32)

    first_half, second_half = list(range(n_half)), list(range(n_half, 2 * n_half))
    local[4].wait()
    local[5].wait()
    near = [(tp, 0, rows), (left_tp, 0, half), (right_tp, half, half)]
    lat[0].wait_recv()
    send_rows(4, raw.at[0, top], 2, top, right_tp)
    lat[1].wait_recv()
    send_rows(5, raw.at[1, low], 2, low, left_tp)
    absorb_keys(jnp.concatenate([latent[...], raw[0, top, :], raw[1, low, :]], axis=0), near, 0)
    pass_on((0, 0), 0)
    local[6].wait()
    absorb_queries(near, 0)

    total = later[...]
    for copy in pc:
        copy.wait_recv()
    for d in range(1, n_sp):
        total = total + later_in[d - 1]
    mods_later[tp] = total
    pd = []
    for i, peer in enumerate((far_tp, left_tp, right_tp)):
        copy = send(mods_later.at[tp], mods_later.at[tp], pd_send.at[i], pd_recv.at[i], {"tp": peer})
        copy.start()
        pd.append(copy)

    early = PAIRS[:6]

    def one(step, carry):
        @pl.when(step == 4)
        def _():
            for copy in pd:
                copy.wait_recv()
            set_ab(1, mods_later)
            local[3].wait()
            x = key_value(modulated(context[...], 1))
            kv[n_sp, share : share + ctx_rows, :] = jnp.where(left, headed(x, kg), x).astype(jnp.bfloat16)

        group_sweep(step, first_half, slots(early, 0), FIRST_EVENTS)
        return carry

    lax.fori_loop(0, len(early), one, 0)

    far = [(left_tp, half, half), (right_tp, 0, half), (far_tp, 0, rows)]
    for i in range(2, 6):
        lat[i].wait_recv()
    absorb_keys(jnp.concatenate([raw[0, low, :], raw[1, top, :], raw[2]], axis=0), far, n_sp)
    pass_on((0, 0), 1)
    absorb_queries(far, n_half)

    def two(step, carry):
        group_sweep(step, second_half, slots(GROUPS, 0), EARLY_EVENTS)
        return carry

    lax.fori_loop(0, len(GROUPS), two, 0)

    def three(step, carry):
        group_sweep(step, second_half, slots(GROUPS, n_sp), LATE_EVENTS)
        return carry

    lax.fori_loop(0, len(GROUPS), three, 0)

    def done(b, o):
        o = (o[:HD] / o[HD : HD + 1]).astype(jnp.bfloat16).astype(jnp.float32)
        both = jnp.concatenate([o[:, :TILE], o[:, TILE:]], axis=0)
        pair, tile = b % n_half // tiles, b % n_half % tiles
        at = b // n_half * share + tile * TILE
        o_tok[at : at + TILE, pair * 2 * HD : (pair + 1) * 2 * HD] = both.T.astype(jnp.bfloat16)

    for slot in range(n_sp):
        kv_ctx[slot * ctx_rows : (slot + 1) * ctx_rows, :] = kv[n_sp + slot, share:, :]
    n_ctx = n_sp * ctx_rows
    span = group * HD
    mine = pl.ds(pl.multiple_of(tp * span, span), span)
    o_copies = []

    def finish(order):
        for t in range(n_ctx // TILE):
            v_t[:HD, t * TILE : (t + 1) * TILE] = kv_ctx[t * TILE : (t + 1) * TILE, :].T[HD:]
        units = [(b, lambda c: kv_ctx[c * KB : (c + 1) * KB, :], 0) for b in order]
        sweep(units, n_ctx, True, done)

    def send_back(at, count, owner, start):
        i = len(o_copies)
        copy = send(
            o_tok.at[at : at + count], o_all.at[start : start + count, mine],
            o_ssem.at[i], o_rsem.at[i], {"tp": owner},
        )
        copy.start()
        o_copies.append(copy)

    finish(second_half)
    send_back(share + rows, rows, far_tp, 0)
    send_back(share, half, left_tp, half)
    send_back(share + half, half, right_tp, 0)

    def four(step, carry):
        group_sweep(step, first_half, last, {})
        return carry

    last = slots(GROUPS, n_sp) + [[place for pair in slots(PAIRS[6:], 0) for place in pair]]
    lax.fori_loop(0, len(last), four, 0)
    finish(first_half)
    send_back(rows, half, left_tp, 0)
    send_back(rows + half, half, right_tp, half)
    o_all[:, mine] = o_tok[0:rows, :]
    local[7].wait()

    def output(where):
        for j in range(n_tp):
            cols = pl.ds(j * chunk, chunk)
            y_j = jnp.dot(o_all[where, :], wout[:, cols], preferred_element_type=jnp.float32)
            first = 2 * per_chunk
            gate = jnp.concatenate([mods_later[j, first + i : first + i + 1] for i in range(per_chunk)], axis=1)
            out[where, cols] = (latent[where, cols].astype(jnp.float32) + gate * y_j).astype(jnp.bfloat16)

    for copy in o_copies:
        copy.wait_recv()
    output(slice(None))

    for copy in lat + pa + pb + pc + pd + o_copies:
        copy.wait_send()
    for index in range(len(flights)):
        flight(index, 0).wait_send()
        flight(index, 1).wait_send()


def on_device(n_sp, n_tp, latent, cond, cond_ctx, context, norm_gain, mod_shift, mod_scale, mod_gate,
              w_query, w_key, w_value, q_gain, k_gain, ctx_lift, w_out):
    _, rows, width = latent.shape
    tokens = rows * n_tp
    ctx_rows = context.shape[1]
    group = w_query.shape[1] // w_key.shape[1]
    keys = tokens + ctx_rows
    row_tab, col_tab = rope_tables(tokens * n_sp // GRID_W)
    chunk = mod_shift.shape[1]
    share = tokens // 2
    n_q = tokens // TILE * group // 2
    bf, f32 = jnp.bfloat16, jnp.float32
    vmem = pl.BlockSpec(memory_space=pltpu.VMEM)
    smem = pl.BlockSpec(memory_space=pltpu.SMEM)
    hbm = pl.BlockSpec(memory_space=pl.ANY)
    dma = pltpu.SemaphoreType.DMA
    out = pl.pallas_call(
        functools.partial(kernel, n_sp, n_tp, group),
        out_shape=jax.ShapeDtypeStruct((rows, width), bf),
        in_specs=[vmem] * 6 + [smem] + [vmem] * 2 + [hbm] * 8,
        out_specs=vmem,
        scratch_shapes=[
            pltpu.VMEM((ctx_rows, width), bf),
            pltpu.VMEM((3,) + mod_shift.shape, bf),
            pltpu.VMEM(w_query.shape, bf),
            pltpu.VMEM((2 * HD, width), bf),
            pltpu.VMEM(w_out.shape, bf),
            pltpu.VMEM((n_tp - 1, rows, width), bf),
            pltpu.VMEM((2 * chunk // TILE, TILE), f32),
            pltpu.VMEM((n_sp - 1, 2 * chunk // TILE, TILE), f32),
            pltpu.VMEM((4 * chunk // TILE, TILE), f32),
            pltpu.VMEM((n_sp - 1, 4 * chunk // TILE, TILE), f32),
            pltpu.VMEM((n_tp, 2 * chunk // TILE, TILE), f32),
            pltpu.VMEM((n_tp, 4 * chunk // TILE, TILE), f32),
            pltpu.VMEM((8, width), f32),
            pltpu.VMEM((2, tokens, 2 * HD), f32),
            pltpu.VMEM((share, width), bf),
            pltpu.VMEM((n_q, 4 * HD, QB), bf),
            pltpu.VMEM((2 * n_sp, share + ctx_rows, 2 * HD), bf),
            pltpu.VMEM((n_sp * ctx_rows, 2 * HD), bf),
            pltpu.VMEM((HD + 16, 2 * tokens), bf),
            pltpu.VMEM((AHEAD + 1, tokens, QB), f32),
            pltpu.VMEM((n_q, HD + 16, QB), f32),
            pltpu.VMEM((n_q, 8, QB), f32),
            pltpu.VMEM((tokens, group * HD), bf),
            pltpu.VMEM((rows, n_tp * group * HD), bf),
            dma((8,)),
            dma((6,)), dma((6,)),
            dma((n_sp - 1,)), dma((n_sp - 1,)),
            dma((n_tp - 1,)), dma((n_tp - 1,)),
            dma((n_sp - 1,)), dma((n_sp - 1,)),
            dma((n_tp - 1,)), dma((n_tp - 1,)),
            dma((2, n_sp - 1)), dma((2, n_sp)),
            dma((5,)), dma((5,)),
        ],
        compiler_params=pltpu.CompilerParams(
            collective_id=0, has_side_effects=True, vmem_limit_bytes=60 * 1024 * 1024,
        ),
    )(
        latent[0], cond, cond_ctx[None], norm_gain.reshape(width // TILE, TILE), q_gain[None], k_gain[None], ctx_lift,
        jnp.asarray(row_tab), jnp.asarray(col_tab),
        context[0], mod_shift, mod_scale, mod_gate, w_query, w_key.T, w_value.T, w_out,
    )
    return out[None]


def solution(mesh):
    placed = (
        P("dp", ("sp", "tp"), None),
        P("dp", "sp"),
        P("sp"),
        P("dp", "sp", None),
        P(),
        P("sp", "tp"),
        P("sp", "tp"),
        P("sp", "tp"),
        P(None, "tp"),
        P(None, "tp"),
        P(None, "tp"),
        P(),
        P(),
        P("tp"),
        P(),
    )
    return jax.shard_map(
        functools.partial(on_device, mesh.shape["sp"], mesh.shape["tp"]),
        mesh=mesh,
        in_specs=placed,
        out_specs=P("dp", ("sp", "tp"), None),
        check_vma=False,
    )
```

```python
import functools

import jax
import jax.numpy as jnp
import numpy as np
from jax import lax
from jax.experimental import pallas as pl
from jax.experimental.pallas import tpu as pltpu
from jax.sharding import PartitionSpec as P

HD = 64
GRID_W = 128
EPS = 1e-06
THETA = 10000.0
MESH = pl.DeviceIdType.MESH
LOG2E = 1.4426950408889634
QB = 256
KB = 256
TILE = 128

PAIRS = (
    ((0, 0), (3, 0)), ((1, 0), (0, 3)), ((0, 1), (2, 0)), ((3, 3), (3, 1)),
    ((1, 3), (1, 1)), ((2, 1), (0, 2)), ((2, 3), (3, 2)), ((1, 2), (2, 2)),
)
GROUPS = (
    ((0, 0), (3, 0), (1, 0), (0, 3)),
    ((0, 1), (2, 0), (3, 3), (3, 1)),
    ((1, 3), (1, 1), (2, 3), (2, 1)),
    ((0, 2), (3, 2), (1, 2), (2, 2)),
)
AHEAD = 3
ONWARD = {
    (0, 0): ((0, 1, (3, 0)), (0, -1, (1, 0)), (1, 1, (0, 3)), (1, -1, (0, 1))),
    (3, 0): ((0, 1, (2, 0)), (1, 1, (3, 3)), (1, -1, (3, 1))),
    (1, 0): ((1, 1, (1, 3)), (1, -1, (1, 1))),
    (2, 0): ((1, 1, (2, 3)), (1, -1, (2, 1))),
    (0, 3): ((1, 1, (0, 2)),),
    (1, 3): ((1, 1, (1, 2)),),
    (3, 1): ((1, -1, (3, 2)),),
    (2, 1): ((1, -1, (2, 2)),),
}


def slot_of(place):
    return place[0] * 4 + place[1]


def slots(groups, base):
    return [[base + slot_of(place) for place in places] for places in groups]


FIRST_EVENTS = {
    0: ((0, (3, 0)), (0, (1, 0)), (0, (0, 3))), 2: ((0, (2, 0)), (0, (3, 1)), (0, (0, 1))), 3: ((0, (3, 3)),),
    4: ((0, (1, 3)), (0, (1, 1))), 5: ((0, (2, 1)), (0, (0, 2))), 6: ((0, (2, 3)), (0, (3, 2))),
    7: ((0, (1, 2)), (0, (2, 2))),
}
EARLY_EVENTS = {
    1: ((1, (3, 0)), (1, (1, 0)), (1, (0, 3))),
    3: ((1, (2, 0)), (1, (3, 3)), (1, (3, 1)), (1, (0, 1))),
}
LATE_EVENTS = {
    0: ((1, (1, 3)), (1, (1, 1))), 1: ((1, (2, 3)), (1, (2, 1))), 2: ((1, (0, 2)), (1, (3, 2))),
    3: ((1, (1, 2)), (1, (2, 2))),
}


def pick(step, values):
    chosen = values[0]
    for i, value in enumerate(values[1:], 1):
        chosen = jnp.where(step == i, value, chosen)
    return chosen


def rope_tables(grid_rows):
    n = HD // 4
    inverse = (np.float32(THETA) ** (-np.arange(n, dtype=np.float32) / np.float32(n))).astype(np.float32)

    def table(count, low):
        angles = (np.arange(count, dtype=np.float32)[:, None] * inverse).astype(np.float32)
        zero = np.zeros((count, 2 * n), np.float32)
        sign = np.tile(np.array([-1.0, 1.0], np.float32), n)
        c = np.repeat(np.cos(angles.astype(np.float64)), 2, axis=1).astype(np.float32)
        s = np.repeat(np.sin(angles.astype(np.float64)), 2, axis=1).astype(np.float32) * sign
        parts = ([c, zero], [s, zero]) if low else ([zero, c], [zero, s])
        return [np.tile(np.concatenate(p, axis=1), (1, 2)) for p in parts]

    return np.stack(table(grid_rows, True)), np.stack(table(GRID_W, False))


def kernel(
    n_sp, n_tp, group,
    latent, cond, cond_ctx, norm_gain, q_gain, k_gain, lift, row_tab, col_tab,
    context_h, mshift_h, mscale_h, mgate_h, wq_h, wk_h, wv_h, wout_h,
    out,
    context, mods_w, wq, wkv, wout,
    raw, part, part_in, later, later_in, mods_all, mods_later, ab, rope, u_buf, q_t, kv, kv_ctx, v_t, s_buf, acc, m_st, o_tok, o_all,
    local_sem, lat_send, lat_recv, pa_send, pa_recv, pb_send, pb_recv, pc_send, pc_recv, pd_send, pd_recv, kv_send, kv_recv, o_ssem, o_rsem,
):
    rows = latent.shape[0]
    half = rows // 2
    width = latent.shape[1]
    chunk = width // n_tp
    tokens = rows * n_tp
    share = tokens // 2
    ctx_rows = context.shape[0]
    sp = lax.axis_index("sp")
    tp = lax.axis_index("tp")
    dp = lax.axis_index("dp")
    left_tp, right_tp, far_tp = (tp + n_tp - 1) % n_tp, (tp + 1) % n_tp, (tp + 2) % n_tp
    peers = (left_tp, right_tp, far_tp)
    sp_order = sorted(range(1, n_sp), key=lambda d: min(d, n_sp - d))

    local = [
        pltpu.make_async_copy(src, dst, local_sem.at[i])
        for i, (src, dst) in enumerate(
            (
                (mshift_h, mods_w.at[0]),
                (mscale_h, mods_w.at[1]),
                (mgate_h, mods_w.at[2]),
                (context_h, context),
                (wk_h, wkv.at[0:HD]),
                (wv_h, wkv.at[HD : 2 * HD]),
                (wq_h, wq),
                (wout_h, wout),
            )
        )
    ]
    for copy in local:
        copy.start()

    barrier = pltpu.get_barrier_semaphore()
    for peer in peers:
        pl.semaphore_signal(barrier, inc=1, device_id={"tp": peer}, device_id_type=MESH)
    for d in range(1, n_sp):
        pl.semaphore_signal(barrier, inc=1, device_id={"sp": (sp + d) % n_sp}, device_id_type=MESH)
    pl.semaphore_wait(barrier, n_tp - 1 + n_sp - 1)

    def send(src, dst, ssem, rsem, device):
        return pltpu.make_async_remote_copy(
            src_ref=src, dst_ref=dst, send_sem=ssem, recv_sem=rsem, device_id=device, device_id_type=MESH
        )

    top, low = pl.ds(0, half), pl.ds(half, half)
    lat = []

    def send_rows(index, src, slot, piece, peer):
        copy = send(src, raw.at[slot, piece], lat_send.at[index], lat_recv.at[index], {"tp": peer})
        copy.start()
        lat.append(copy)

    send_rows(0, latent.at[top], 0, top, right_tp)
    send_rows(1, latent.at[low], 1, low, left_tp)

    act = jnp.concatenate([cond[...], cond_ctx[...]], axis=0).astype(jnp.float32)
    act = (act / (1.0 + jnp.exp(-act))).astype(jnp.bfloat16)
    act = jnp.concatenate([act, jnp.zeros((14, act.shape[1]), jnp.bfloat16)], axis=0)
    for i in range(3):
        local[i].wait()
    sums = [jnp.dot(act, mods_w[i], preferred_element_type=jnp.float32)[0:2] for i in range(3)]
    per_chunk = chunk // TILE

    def stacked(rows_of):
        return jnp.concatenate(
            [r[:, i * TILE : (i + 1) * TILE] for r in rows_of for i in range(per_chunk)], axis=0
        )

    part[...] = stacked([sums[0][0:1], sums[1][0:1], sums[0][1:2], sums[1][1:2]])
    later[...] = stacked([sums[2][0:1], jnp.zeros((1, chunk), jnp.float32)])
    pa, pc = [], []
    for out_list, src, dst, ssem, rsem in (
        (pa, part, part_in, pa_send, pa_recv), (pc, later, later_in, pc_send, pc_recv)
    ):
        for d in sp_order:
            copy = send(src, dst.at[d - 1], ssem.at[d - 1], rsem.at[d - 1], {"sp": (sp + d) % n_sp})
            copy.start()
            out_list.append(copy)

    groups = tokens // GRID_W
    for i in range(2):
        for g in range(groups):
            rope[i, pl.ds(g * GRID_W, GRID_W), :] = (
                row_tab[i, pl.ds(sp * groups + g, 1), :] + col_tab[i, :, :]
            )

    total = part[...]
    for copy in pa:
        copy.wait_recv()
    for d in range(1, n_sp):
        total = total + part_in[d - 1]
    mods_all[tp] = total
    pb = []
    for i, peer in enumerate((far_tp, left_tp, right_tp)):
        copy = send(mods_all.at[tp], mods_all.at[tp], pb_send.at[i], pb_recv.at[i], {"tp": peer})
        copy.start()
        pb.append(copy)
    send_rows(2, latent.at[low], 0, low, right_tp)
    send_rows(3, latent.at[top], 1, top, left_tp)

    for copy in pb:
        copy.wait_recv()

    for row in range(2):
        for j in range(n_tp):
            block = mods_all[j, 2 * row * per_chunk : 2 * (row + 1) * per_chunk]
            for i in range(per_chunk):
                at = j * chunk + i * TILE
                gain = norm_gain[at // TILE : at // TILE + 1, :].astype(jnp.float32)
                ab[row : row + 1, at : at + TILE] = gain * (1.0 + block[per_chunk + i : per_chunk + i + 1])
                ab[row + 2 : row + 3, at : at + TILE] = block[i : i + 1]

    lane = lax.broadcasted_iota(jnp.int32, (1, 2 * HD), 1)
    even = lane % 2 == 0
    left = lane < HD
    ones = (
        (lax.broadcasted_iota(jnp.int32, (2 * HD, 2 * HD), 0) < HD)
        == (lax.broadcasted_iota(jnp.int32, (2 * HD, 2 * HD), 1) < HD)
    ).astype(jnp.bfloat16)
    qg = jnp.concatenate([q_gain[...]] * 2, axis=1).astype(jnp.float32)
    kg = jnp.concatenate([k_gain[...]] * 2, axis=1).astype(jnp.float32)
    factor = LOG2E * HD ** (-0.5)

    def modulated(block, row):
        values = block.astype(jnp.float32)
        scale = lax.rsqrt(jnp.mean(values * values, axis=-1, keepdims=True) + EPS)
        return (values * scale * ab[row : row + 1, :] + ab[row + 2 : row + 3, :]).astype(jnp.bfloat16)

    def headed(x, g):
        square = x * x
        high = square.astype(jnp.bfloat16)
        rest = (square - high.astype(jnp.float32)).astype(jnp.bfloat16)
        mean = (
            jnp.dot(high, ones, preferred_element_type=jnp.float32)
            + jnp.dot(rest, ones, preferred_element_type=jnp.float32)
        ) * (1.0 / HD)
        return x * lax.rsqrt(mean + EPS) * g

    def turned(x, cosine, sine):
        partner = jnp.where(even, pltpu.roll(x, 2 * HD - 1, 1), pltpu.roll(x, 1, 1))
        return x * cosine + partner * sine

    def key_value(u):
        return lax.dot_general(u, wkv[...], (((1,), (1,)), ((), ())), preferred_element_type=jnp.float32)

    def angles(owner, start, count):
        where = pl.ds(pl.multiple_of(owner * rows + start, half), count)
        return rope[0, where, :], rope[1, where, :]

    def tables_of(pieces):
        tables = [angles(*piece) for piece in pieces]
        return [jnp.concatenate([t[i] for t in tables], axis=0) for i in range(2)]

    def absorb_keys(block, pieces, slot):
        u = modulated(block, 0)
        u_buf[...] = u
        cosine, sine = tables_of(pieces)
        x = key_value(u)
        kv[slot, :share, :] = jnp.where(left, turned(headed(x, kg), cosine, sine), x).astype(jnp.bfloat16)

    def absorb_queries(pieces, first):
        cosine, sine = tables_of(pieces)
        raw_q = jnp.dot(u_buf[...], wq[...], preferred_element_type=jnp.float32)
        none = jnp.zeros((HD, QB), jnp.bfloat16)
        for pair in range(group // 2):
            x = raw_q[:, pair * 2 * HD : (pair + 1) * 2 * HD]
            x = turned(headed(x, qg), cosine, sine).astype(jnp.bfloat16).astype(jnp.float32) * factor
            for tile in range(tiles):
                t = x[tile * TILE : (tile + 1) * TILE, :].T
                t = jnp.concatenate([t[:HD], t[HD:]], axis=1)
                high = t.astype(jnp.bfloat16)
                rest = (t - high.astype(jnp.float32)).astype(jnp.bfloat16)
                q_t[first + pair * tiles + tile] = jnp.concatenate([high, none, rest, none], axis=0)

    side = int(round(n_sp ** 0.5))
    y, z = sp % side, sp // side

    def neighbour(axis, step):
        along_y = z * side + (y + step + side) % side
        along_z = (z + step + side) % side * side + y
        return jnp.where(dp == axis, along_y, along_z)

    flights = [(place, hop) for place in ONWARD for hop in ONWARD[place]]

    def flight(index, which):
        place, (axis, step, target) = flights[index]
        piece = pl.ds(0, share + which * ctx_rows)
        base = which * n_sp
        return send(
            kv.at[base + slot_of(place), piece], kv.at[base + slot_of(target), piece],
            kv_send.at[which, index], kv_recv.at[which, slot_of(target)],
            {"sp": neighbour(axis, step)},
        )

    def pass_on(place, which):
        for index in range(len(flights)):
            if flights[index][0] == place:
                flight(index, which).start()

    def arrived(place, which):
        for index in range(len(flights)):
            if flights[index][1][2] == place:
                flight(index, which).wait_recv()

    tiles = share // TILE
    n_half = tiles * group // 2

    def sweep(units, n_keys, lifted, done):
        chunks = n_keys // KB
        tops, sums = {}, {}

        def scores(i, c):
            b, load, at = units[i]
            piece = load(c)
            s = jnp.dot(
                jnp.concatenate([piece, piece], axis=1), q_t[b], preferred_element_type=jnp.float32
            )
            if lifted:
                pair = b % n_half // tiles
                wide = lax.broadcasted_iota(jnp.int32, (1, QB), 1)
                s = s + jnp.where(wide < TILE, lift[2 * pair], lift[2 * pair + 1]) * LOG2E
            s_buf[i % (AHEAD + 1), c * KB : (c + 1) * KB, :] = s
            high = jnp.max(s.reshape(KB // 8, 8, QB), axis=0)
            tops[i] = jnp.maximum(tops[i], high) if i in tops else high

        for i in range(min(AHEAD, len(units))):
            for c in range(chunks):
                scores(i, c)
        for i, (b, load, at) in enumerate(units):
            m_old = m_st[b]
            m = jnp.maximum(m_old, jnp.max(tops.pop(i), axis=0, keepdims=True))
            m_st[b] = m
            alpha = jnp.exp2(m_old - m)
            o = None
            for c in range(chunks):
                if i + AHEAD < len(units):
                    scores(i + AHEAD, c)
                x = s_buf[i % (AHEAD + 1), c * KB : (c + 1) * KB, :].reshape(KB // 8, 8, QB) - m[None]
                p = jnp.exp2(x).reshape(KB, QB).astype(jnp.bfloat16)
                values = v_t[:, at + c * KB : at + (c + 1) * KB]
                term = jnp.dot(values, p, preferred_element_type=jnp.float32)
                o = term if o is None else o + term
            o = acc[b] * alpha[0:1] + o
            if done is None:
                acc[b] = o
            else:
                done(b, o)

    def group_sweep(step, order, table, events):
        for k in events:
            @pl.when(step == k)
            def _(k=k):
                for which, place in events[k]:
                    arrived(place, which)
                    pass_on(place, which)

        many = len(table[0])
        ids = [pick(step, [places[i] for places in table]) for i in range(many)]

        def tile_at(t):
            return kv[ids[t // tiles], t % tiles * TILE : (t % tiles + 1) * TILE, :]

        for t in range(many * tiles):
            v_t[:HD, t * TILE : (t + 1) * TILE] = tile_at(t).T[HD:]
        per = KB // TILE

        def loader(base):
            return lambda c: jnp.concatenate([tile_at(base + c * per + i) for i in range(per)], axis=0)

        units = [(b, loader(2 * tiles * pair), 2 * share * pair) for pair in range(many // 2) for b in order]
        sweep(units, 2 * share, False, None)

    v_t[HD:, :] = jnp.ones((v_t.shape[0] - HD, v_t.shape[1]), jnp.bfloat16)
    acc[...] = jnp.zeros_like(acc)
    m_st[...] = jnp.full(m_st.shape, -1e30, jnp.float32)

    first_half, second_half = list(range(n_half)), list(range(n_half, 2 * n_half))
    local[4].wait()
    local[5].wait()
    near = [(tp, 0, rows), (left_tp, 0, half), (right_tp, half, half)]
    lat[0].wait_recv()
    send_rows(4, raw.at[0, top], 2, top, right_tp)
    lat[1].wait_recv()
    send_rows(5, raw.at[1, low], 2, low, left_tp)
    absorb_keys(jnp.concatenate([latent[...], raw[0, top, :], raw[1, low, :]], axis=0), near, 0)
    pass_on((0, 0), 0)
    local[6].wait()
    absorb_queries(near, 0)

    total = later[...]
    for copy in pc:
        copy.wait_recv()
    for d in range(1, n_sp):
        total = total + later_in[d - 1]
    mods_later[tp] = total
    pd = []
    for i, peer in enumerate((far_tp, left_tp, right_tp)):
        copy = send(mods_later.at[tp], mods_later.at[tp], pd_send.at[i], pd_recv.at[i], {"tp": peer})
        copy.start()
        pd.append(copy)

    local[3].wait()
    x = key_value(modulated(context[...], 1))
    kv[n_sp, share : share + ctx_rows, :] = jnp.where(left, headed(x, kg), x).astype(jnp.bfloat16)

    def one(step, carry):
        group_sweep(step, first_half, slots(PAIRS, 0), FIRST_EVENTS)
        return carry

    lax.fori_loop(0, len(PAIRS), one, 0)

    far = [(left_tp, half, half), (right_tp, 0, half), (far_tp, 0, rows)]
    for i in range(2, 6):
        lat[i].wait_recv()
    absorb_keys(jnp.concatenate([raw[0, low, :], raw[1, top, :], raw[2]], axis=0), far, n_sp)
    pass_on((0, 0), 1)
    absorb_queries(far, n_half)

    def two(step, carry):
        group_sweep(step, second_half, slots(GROUPS, 0), EARLY_EVENTS)
        return carry

    lax.fori_loop(0, len(GROUPS), two, 0)

    def three(step, carry):
        group_sweep(step, second_half, slots(GROUPS, n_sp), LATE_EVENTS)
        return carry

    lax.fori_loop(0, len(GROUPS), three, 0)

    def done(b, o):
        o = (o[:HD] / o[HD : HD + 1]).astype(jnp.bfloat16).astype(jnp.float32)
        both = jnp.concatenate([o[:, :TILE], o[:, TILE:]], axis=0)
        pair, tile = b % n_half // tiles, b % n_half % tiles
        at = b // n_half * share + tile * TILE
        o_tok[at : at + TILE, pair * 2 * HD : (pair + 1) * 2 * HD] = both.T.astype(jnp.bfloat16)

    for slot in range(n_sp):
        kv_ctx[slot * ctx_rows : (slot + 1) * ctx_rows, :] = kv[n_sp + slot, share:, :]
    n_ctx = n_sp * ctx_rows
    span = group * HD
    mine = pl.ds(pl.multiple_of(tp * span, span), span)
    o_copies = []

    def finish(order):
        for t in range(n_ctx // TILE):
            v_t[:HD, t * TILE : (t + 1) * TILE] = kv_ctx[t * TILE : (t + 1) * TILE, :].T[HD:]
        units = [(b, lambda c: kv_ctx[c * KB : (c + 1) * KB, :], 0) for b in order]
        sweep(units, n_ctx, True, done)

    def send_back(at, count, owner, start):
        i = len(o_copies)
        copy = send(
            o_tok.at[at : at + count], o_all.at[start : start + count, mine],
            o_ssem.at[i], o_rsem.at[i], {"tp": owner},
        )
        copy.start()
        o_copies.append(copy)

    finish(second_half)
    send_back(share + rows, rows, far_tp, 0)
    send_back(share, half, left_tp, half)
    send_back(share + half, half, right_tp, 0)

    mixed_blocks = [b for b in first_half if b % tiles > 0]
    own_blocks = [b for b in first_half if b % tiles == 0]

    def four(step, carry):
        group_sweep(step, mixed_blocks, slots(GROUPS, n_sp), {})
        return carry

    lax.fori_loop(0, len(GROUPS), four, 0)
    finish(mixed_blocks)
    send_back(rows, half, left_tp, 0)
    send_back(rows + half, half, right_tp, half)

    wide = slots([GROUPS[0] + GROUPS[1], GROUPS[2] + GROUPS[3]], n_sp)

    def five(step, carry):
        group_sweep(step, own_blocks, wide, {})
        return carry

    lax.fori_loop(0, len(wide), five, 0)
    finish(own_blocks)
    o_all[:, mine] = o_tok[0:rows, :]
    local[7].wait()

    def output(where):
        for j in range(n_tp):
            cols = pl.ds(j * chunk, chunk)
            y_j = jnp.dot(o_all[where, :], wout[:, cols], preferred_element_type=jnp.float32)
            gate = jnp.concatenate([mods_later[j, i : i + 1] for i in range(per_chunk)], axis=1)
            out[where, cols] = (latent[where, cols].astype(jnp.float32) + gate * y_j).astype(jnp.bfloat16)

    for copy in pd + o_copies:
        copy.wait_recv()
    output(slice(None))

    for copy in lat + pa + pb + pc + pd + o_copies:
        copy.wait_send()
    for index in range(len(flights)):
        flight(index, 0).wait_send()
        flight(index, 1).wait_send()


def on_device(n_sp, n_tp, latent, cond, cond_ctx, context, norm_gain, mod_shift, mod_scale, mod_gate,
              w_query, w_key, w_value, q_gain, k_gain, ctx_lift, w_out):
    _, rows, width = latent.shape
    tokens = rows * n_tp
    ctx_rows = context.shape[1]
    group = w_query.shape[1] // w_key.shape[1]
    keys = tokens + ctx_rows
    row_tab, col_tab = rope_tables(tokens * n_sp // GRID_W)
    chunk = mod_shift.shape[1]
    share = tokens // 2
    n_q = tokens // TILE * group // 2
    bf, f32 = jnp.bfloat16, jnp.float32
    vmem = pl.BlockSpec(memory_space=pltpu.VMEM)
    smem = pl.BlockSpec(memory_space=pltpu.SMEM)
    hbm = pl.BlockSpec(memory_space=pl.ANY)
    dma = pltpu.SemaphoreType.DMA
    out = pl.pallas_call(
        functools.partial(kernel, n_sp, n_tp, group),
        out_shape=jax.ShapeDtypeStruct((rows, width), bf),
        in_specs=[vmem] * 6 + [smem] + [vmem] * 2 + [hbm] * 8,
        out_specs=vmem,
        scratch_shapes=[
            pltpu.VMEM((ctx_rows, width), bf),
            pltpu.VMEM((3,) + mod_shift.shape, bf),
            pltpu.VMEM(w_query.shape, bf),
            pltpu.VMEM((2 * HD, width), bf),
            pltpu.VMEM(w_out.shape, bf),
            pltpu.VMEM((n_tp - 1, rows, width), bf),
            pltpu.VMEM((4 * chunk // TILE, TILE), f32),
            pltpu.VMEM((n_sp - 1, 4 * chunk // TILE, TILE), f32),
            pltpu.VMEM((2 * chunk // TILE, TILE), f32),
            pltpu.VMEM((n_sp - 1, 2 * chunk // TILE, TILE), f32),
            pltpu.VMEM((n_tp, 4 * chunk // TILE, TILE), f32),
            pltpu.VMEM((n_tp, 2 * chunk // TILE, TILE), f32),
            pltpu.VMEM((8, width), f32),
            pltpu.VMEM((2, tokens, 2 * HD), f32),
            pltpu.VMEM((share, width), bf),
            pltpu.VMEM((n_q, 4 * HD, QB), bf),
            pltpu.VMEM((2 * n_sp, share + ctx_rows, 2 * HD), bf),
            pltpu.VMEM((n_sp * ctx_rows, 2 * HD), bf),
            pltpu.VMEM((HD + 16, 4 * tokens), bf),
            pltpu.VMEM((AHEAD + 1, tokens, QB), f32),
            pltpu.VMEM((n_q, HD + 16, QB), f32),
            pltpu.VMEM((n_q, 8, QB), f32),
            pltpu.VMEM((tokens, group * HD), bf),
            pltpu.VMEM((rows, n_tp * group * HD), bf),
            dma((8,)),
            dma((6,)), dma((6,)),
            dma((n_sp - 1,)), dma((n_sp - 1,)),
            dma((n_tp - 1,)), dma((n_tp - 1,)),
            dma((n_sp - 1,)), dma((n_sp - 1,)),
            dma((n_tp - 1,)), dma((n_tp - 1,)),
            dma((2, n_sp - 1)), dma((2, n_sp)),
            dma((5,)), dma((5,)),
        ],
        compiler_params=pltpu.CompilerParams(
            collective_id=0, has_side_effects=True, vmem_limit_bytes=60 * 1024 * 1024,
        ),
    )(
        latent[0], cond, cond_ctx[None], norm_gain.reshape(width // TILE, TILE), q_gain[None], k_gain[None], ctx_lift,
        jnp.asarray(row_tab), jnp.asarray(col_tab),
        context[0], mod_shift, mod_scale, mod_gate, w_query, w_key.T, w_value.T, w_out,
    )
    return out[None]


def solution(mesh):
    placed = (
        P("dp", ("sp", "tp"), None),
        P("dp", "sp"),
        P("sp"),
        P("dp", "sp", None),
        P(),
        P("sp", "tp"),
        P("sp", "tp"),
        P("sp", "tp"),
        P(None, "tp"),
        P(None, "tp"),
        P(None, "tp"),
        P(),
        P(),
        P("tp"),
        P(),
    )
    return jax.shard_map(
        functools.partial(on_device, mesh.shape["sp"], mesh.shape["tp"]),
        mesh=mesh,
        in_specs=placed,
        out_specs=P("dp", ("sp", "tp"), None),
        check_vma=False,
    )
```

```python
import functools

import jax
import jax.numpy as jnp
import numpy as np
from jax import lax
from jax.experimental import pallas as pl
from jax.experimental.pallas import tpu as pltpu
from jax.sharding import PartitionSpec as P

HD = 64
GRID_W = 128
EPS = 1e-06
THETA = 10000.0
MESH = pl.DeviceIdType.MESH
LOG2E = 1.4426950408889634
QB = 256
KB = 256
TILE = 128

PAIRS = (
    ((0, 0), (3, 0)), ((1, 0), (0, 3)), ((0, 1), (2, 0)), ((3, 3), (3, 1)),
    ((1, 3), (1, 1)), ((2, 1), (0, 2)), ((2, 3), (3, 2)), ((1, 2), (2, 2)),
)
GROUPS = (
    ((0, 0), (3, 0), (1, 0), (0, 3)),
    ((0, 1), (2, 0), (3, 3), (3, 1)),
    ((1, 3), (1, 1), (2, 3), (2, 1)),
    ((0, 2), (3, 2), (1, 2), (2, 2)),
)
AHEAD = 3
ONWARD = {
    (0, 0): ((0, 1, (3, 0)), (0, -1, (1, 0)), (1, 1, (0, 3)), (1, -1, (0, 1))),
    (3, 0): ((0, 1, (2, 0)), (1, 1, (3, 3)), (1, -1, (3, 1))),
    (1, 0): ((1, 1, (1, 3)), (1, -1, (1, 1))),
    (2, 0): ((1, 1, (2, 3)), (1, -1, (2, 1))),
    (0, 3): ((1, 1, (0, 2)),),
    (1, 3): ((1, 1, (1, 2)),),
    (3, 1): ((1, -1, (3, 2)),),
    (2, 1): ((1, -1, (2, 2)),),
}


def slot_of(place):
    return place[0] * 4 + place[1]


def slots(groups, base):
    return [[base + slot_of(place) for place in places] for places in groups]


FIRST_EVENTS = {
    0: ((0, (3, 0)), (0, (1, 0)), (0, (0, 3))), 2: ((0, (2, 0)), (0, (3, 1)), (0, (0, 1))), 3: ((0, (3, 3)),),
    4: ((0, (1, 3)), (0, (1, 1))), 5: ((0, (2, 1)), (0, (0, 2))), 6: ((0, (2, 3)), (0, (3, 2))),
    7: ((0, (1, 2)), (0, (2, 2))),
}
EARLY_EVENTS = {
    1: ((1, (3, 0)), (1, (1, 0)), (1, (0, 3))),
    3: ((1, (2, 0)), (1, (3, 3)), (1, (3, 1)), (1, (0, 1))),
}
LATE_EVENTS = {
    0: ((1, (1, 3)), (1, (1, 1))), 1: ((1, (2, 3)), (1, (2, 1))), 2: ((1, (0, 2)), (1, (3, 2))),
    3: ((1, (1, 2)), (1, (2, 2))),
}


def pick(step, values):
    chosen = values[0]
    for i, value in enumerate(values[1:], 1):
        chosen = jnp.where(step == i, value, chosen)
    return chosen


def rope_tables(grid_rows):
    n = HD // 4
    inverse = (np.float32(THETA) ** (-np.arange(n, dtype=np.float32) / np.float32(n))).astype(np.float32)

    def table(count, low):
        angles = (np.arange(count, dtype=np.float32)[:, None] * inverse).astype(np.float32)
        zero = np.zeros((count, 2 * n), np.float32)
        sign = np.tile(np.array([-1.0, 1.0], np.float32), n)
        c = np.repeat(np.cos(angles.astype(np.float64)), 2, axis=1).astype(np.float32)
        s = np.repeat(np.sin(angles.astype(np.float64)), 2, axis=1).astype(np.float32) * sign
        parts = ([c, zero], [s, zero]) if low else ([zero, c], [zero, s])
        return [np.tile(np.concatenate(p, axis=1), (1, 2)) for p in parts]

    return np.stack(table(grid_rows, True)), np.stack(table(GRID_W, False))


def kernel(
    n_sp, n_tp, group,
    latent, cond, cond_ctx, norm_gain, q_gain, k_gain, lift, row_tab, col_tab,
    context_h, mshift_h, mscale_h, mgate_h, wq_h, wk_h, wv_h, wout_h,
    out,
    context, mods_w, wq, wkv, wout,
    raw, part, part_in, later, later_in, mods_all, mods_later, ab, rope, u_buf, q_t, kv, kv_ctx, v_t, s_buf, acc, m_st, o_tok, o_all,
    local_sem, lat_send, lat_recv, pa_send, pa_recv, pb_send, pb_recv, pc_send, pc_recv, pd_send, pd_recv, kv_send, kv_recv, o_ssem, o_rsem,
):
    rows = latent.shape[0]
    half = rows // 2
    width = latent.shape[1]
    chunk = width // n_tp
    tokens = rows * n_tp
    share = tokens // 2
    ctx_rows = context.shape[0]
    sp = lax.axis_index("sp")
    tp = lax.axis_index("tp")
    dp = lax.axis_index("dp")
    left_tp, right_tp, far_tp = (tp + n_tp - 1) % n_tp, (tp + 1) % n_tp, (tp + 2) % n_tp
    peers = (left_tp, right_tp, far_tp)
    sp_order = sorted(range(1, n_sp), key=lambda d: min(d, n_sp - d))

    local = [
        pltpu.make_async_copy(src, dst, local_sem.at[i])
        for i, (src, dst) in enumerate(
            (
                (mshift_h, mods_w.at[0]),
                (mscale_h, mods_w.at[1]),
                (mgate_h, mods_w.at[2]),
                (context_h, context),
                (wk_h, wkv.at[0:HD]),
                (wv_h, wkv.at[HD : 2 * HD]),
                (wq_h, wq),
                (wout_h, wout),
            )
        )
    ]
    for copy in local:
        copy.start()

    barrier = pltpu.get_barrier_semaphore()
    for peer in peers:
        pl.semaphore_signal(barrier, inc=1, device_id={"tp": peer}, device_id_type=MESH)
    for d in range(1, n_sp):
        pl.semaphore_signal(barrier, inc=1, device_id={"sp": (sp + d) % n_sp}, device_id_type=MESH)
    pl.semaphore_wait(barrier, n_tp - 1 + n_sp - 1)

    def send(src, dst, ssem, rsem, device):
        return pltpu.make_async_remote_copy(
            src_ref=src, dst_ref=dst, send_sem=ssem, recv_sem=rsem, device_id=device, device_id_type=MESH
        )

    top, low = pl.ds(0, half), pl.ds(half, half)
    lat = []

    def send_rows(index, src, slot, piece, peer):
        copy = send(src, raw.at[slot, piece], lat_send.at[index], lat_recv.at[index], {"tp": peer})
        copy.start()
        lat.append(copy)

    send_rows(0, latent.at[top], 0, top, right_tp)
    send_rows(1, latent.at[low], 1, low, left_tp)

    act = jnp.concatenate([cond[...], cond_ctx[...]], axis=0).astype(jnp.float32)
    act = (act / (1.0 + jnp.exp(-act))).astype(jnp.bfloat16)
    act = jnp.concatenate([act, jnp.zeros((14, act.shape[1]), jnp.bfloat16)], axis=0)
    for i in range(3):
        local[i].wait()
    sums = [jnp.dot(act, mods_w[i], preferred_element_type=jnp.float32)[0:2] for i in range(3)]
    per_chunk = chunk // TILE

    def stacked(rows_of):
        return jnp.concatenate(
            [r[:, i * TILE : (i + 1) * TILE] for r in rows_of for i in range(per_chunk)], axis=0
        )

    part[...] = stacked([sums[0][0:1], sums[1][0:1], sums[0][1:2], sums[1][1:2]])
    later[...] = stacked([sums[2][0:1], jnp.zeros((1, chunk), jnp.float32)])
    pa, pc = [], []
    for out_list, src, dst, ssem, rsem in (
        (pa, part, part_in, pa_send, pa_recv), (pc, later, later_in, pc_send, pc_recv)
    ):
        for d in sp_order:
            copy = send(src, dst.at[d - 1], ssem.at[d - 1], rsem.at[d - 1], {"sp": (sp + d) % n_sp})
            copy.start()
            out_list.append(copy)

    groups = tokens // GRID_W
    for i in range(2):
        for g in range(groups):
            rope[i, pl.ds(g * GRID_W, GRID_W), :] = (
                row_tab[i, pl.ds(sp * groups + g, 1), :] + col_tab[i, :, :]
            )

    total = part[...]
    for copy in pa:
        copy.wait_recv()
    for d in range(1, n_sp):
        total = total + part_in[d - 1]
    mods_all[tp] = total
    pb = []
    for i, peer in enumerate((far_tp, left_tp, right_tp)):
        copy = send(mods_all.at[tp], mods_all.at[tp], pb_send.at[i], pb_recv.at[i], {"tp": peer})
        copy.start()
        pb.append(copy)
    send_rows(2, latent.at[low], 0, low, right_tp)
    send_rows(3, latent.at[top], 1, top, left_tp)

    for copy in pb:
        copy.wait_recv()

    for row in range(2):
        for j in range(n_tp):
            block = mods_all[j, 2 * row * per_chunk : 2 * (row + 1) * per_chunk]
            for i in range(per_chunk):
                at = j * chunk + i * TILE
                gain = norm_gain[at // TILE : at // TILE + 1, :].astype(jnp.float32)
                ab[row : row + 1, at : at + TILE] = gain * (1.0 + block[per_chunk + i : per_chunk + i + 1])
                ab[row + 2 : row + 3, at : at + TILE] = block[i : i + 1]

    lane = lax.broadcasted_iota(jnp.int32, (1, 2 * HD), 1)
    even = lane % 2 == 0
    left = lane < HD
    ones = (
        (lax.broadcasted_iota(jnp.int32, (2 * HD, 2 * HD), 0) < HD)
        == (lax.broadcasted_iota(jnp.int32, (2 * HD, 2 * HD), 1) < HD)
    ).astype(jnp.bfloat16)
    qg = jnp.concatenate([q_gain[...]] * 2, axis=1).astype(jnp.float32)
    kg = jnp.concatenate([k_gain[...]] * 2, axis=1).astype(jnp.float32)
    factor = LOG2E * HD ** (-0.5)

    def modulated(block, row):
        values = block.astype(jnp.float32)
        scale = lax.rsqrt(jnp.mean(values * values, axis=-1, keepdims=True) + EPS)
        return (values * scale * ab[row : row + 1, :] + ab[row + 2 : row + 3, :]).astype(jnp.bfloat16)

    def headed(x, g):
        square = x * x
        high = square.astype(jnp.bfloat16)
        rest = (square - high.astype(jnp.float32)).astype(jnp.bfloat16)
        mean = (
            jnp.dot(high, ones, preferred_element_type=jnp.float32)
            + jnp.dot(rest, ones, preferred_element_type=jnp.float32)
        ) * (1.0 / HD)
        return x * lax.rsqrt(mean + EPS) * g

    def turned(x, cosine, sine):
        partner = jnp.where(even, pltpu.roll(x, 2 * HD - 1, 1), pltpu.roll(x, 1, 1))
        return x * cosine + partner * sine

    def key_value(u):
        return lax.dot_general(u, wkv[...], (((1,), (1,)), ((), ())), preferred_element_type=jnp.float32)

    def angles(owner, start, count):
        where = pl.ds(pl.multiple_of(owner * rows + start, half), count)
        return rope[0, where, :], rope[1, where, :]

    def tables_of(pieces):
        tables = [angles(*piece) for piece in pieces]
        return [jnp.concatenate([t[i] for t in tables], axis=0) for i in range(2)]

    def absorb_keys(block, pieces, slot):
        u = modulated(block, 0)
        u_buf[...] = u
        cosine, sine = tables_of(pieces)
        x = key_value(u)
        kv[slot, :share, :] = jnp.where(left, turned(headed(x, kg), cosine, sine), x).astype(jnp.bfloat16)

    def absorb_queries(pieces, first):
        cosine, sine = tables_of(pieces)
        raw_q = jnp.dot(u_buf[...], wq[...], preferred_element_type=jnp.float32)
        none = jnp.zeros((HD, QB), jnp.bfloat16)
        for pair in range(group // 2):
            x = raw_q[:, pair * 2 * HD : (pair + 1) * 2 * HD]
            x = turned(headed(x, qg), cosine, sine).astype(jnp.bfloat16).astype(jnp.float32) * factor
            for tile in range(tiles):
                t = x[tile * TILE : (tile + 1) * TILE, :].T
                t = jnp.concatenate([t[:HD], t[HD:]], axis=1)
                high = t.astype(jnp.bfloat16)
                rest = (t - high.astype(jnp.float32)).astype(jnp.bfloat16)
                q_t[first + pair * tiles + tile] = jnp.concatenate([high, none, rest, none], axis=0)

    side = int(round(n_sp ** 0.5))
    y, z = sp % side, sp // side

    def neighbour(axis, step):
        along_y = z * side + (y + step + side) % side
        along_z = (z + step + side) % side * side + y
        return jnp.where(dp == axis, along_y, along_z)

    flights = [(place, hop) for place in ONWARD for hop in ONWARD[place]]

    def flight(index, which):
        place, (axis, step, target) = flights[index]
        piece = pl.ds(0, share + which * ctx_rows)
        base = which * n_sp
        return send(
            kv.at[base + slot_of(place), piece], kv.at[base + slot_of(target), piece],
            kv_send.at[which, index], kv_recv.at[which, slot_of(target)],
            {"sp": neighbour(axis, step)},
        )

    def pass_on(place, which):
        for index in range(len(flights)):
            if flights[index][0] == place:
                flight(index, which).start()

    def arrived(place, which):
        for index in range(len(flights)):
            if flights[index][1][2] == place:
                flight(index, which).wait_recv()

    tiles = share // TILE
    n_half = tiles * group // 2

    def sweep(units, n_keys, lifted, done):
        chunks = n_keys // KB
        tops, sums = {}, {}

        def scores(i, c):
            b, load, at = units[i]
            piece = load(c)
            s = jnp.dot(
                jnp.concatenate([piece, piece], axis=1), q_t[b], preferred_element_type=jnp.float32
            )
            if lifted:
                pair = b % n_half // tiles
                wide = lax.broadcasted_iota(jnp.int32, (1, QB), 1)
                s = s + jnp.where(wide < TILE, lift[2 * pair], lift[2 * pair + 1]) * LOG2E
            s_buf[i % (AHEAD + 1), c * KB : (c + 1) * KB, :] = s
            high = jnp.max(s.reshape(KB // 8, 8, QB), axis=0)
            tops[i] = jnp.maximum(tops[i], high) if i in tops else high

        for i in range(min(AHEAD, len(units))):
            for c in range(chunks):
                scores(i, c)
        for i, (b, load, at) in enumerate(units):
            m_old = m_st[b]
            m = jnp.maximum(m_old, jnp.max(tops.pop(i), axis=0, keepdims=True))
            m_st[b] = m
            alpha = jnp.exp2(m_old - m)
            o = None
            for c in range(chunks):
                if i + AHEAD < len(units):
                    scores(i + AHEAD, c)
                x = s_buf[i % (AHEAD + 1), c * KB : (c + 1) * KB, :].reshape(KB // 8, 8, QB) - m[None]
                p = jnp.exp2(x).reshape(KB, QB).astype(jnp.bfloat16)
                values = v_t[:, at + c * KB : at + (c + 1) * KB]
                term = jnp.dot(values, p, preferred_element_type=jnp.float32)
                o = term if o is None else o + term
            o = acc[b] * alpha[0:1] + o
            if done is None:
                acc[b] = o
            else:
                done(b, o)

    def group_sweep(step, order, table, events):
        for k in events:
            @pl.when(step == k)
            def _(k=k):
                for which, place in events[k]:
                    arrived(place, which)
                    pass_on(place, which)

        many = len(table[0])
        ids = [pick(step, [places[i] for places in table]) for i in range(many)]

        def tile_at(t):
            return kv[ids[t // tiles], t % tiles * TILE : (t % tiles + 1) * TILE, :]

        for t in range(many * tiles):
            v_t[:HD, t * TILE : (t + 1) * TILE] = tile_at(t).T[HD:]
        per = KB // TILE

        def loader(base):
            return lambda c: jnp.concatenate([tile_at(base + c * per + i) for i in range(per)], axis=0)

        units = [(b, loader(2 * tiles * pair), 2 * share * pair) for pair in range(many // 2) for b in order]
        sweep(units, 2 * share, False, None)

    v_t[HD:, :] = jnp.ones((v_t.shape[0] - HD, v_t.shape[1]), jnp.bfloat16)
    acc[...] = jnp.zeros_like(acc)
    m_st[...] = jnp.full(m_st.shape, -1e30, jnp.float32)

    first_half, second_half = list(range(n_half)), list(range(n_half, 2 * n_half))
    local[4].wait()
    local[5].wait()
    near = [(tp, 0, rows), (left_tp, 0, half), (right_tp, half, half)]
    lat[0].wait_recv()
    send_rows(4, raw.at[0, top], 2, top, right_tp)
    lat[1].wait_recv()
    send_rows(5, raw.at[1, low], 2, low, left_tp)
    absorb_keys(jnp.concatenate([latent[...], raw[0, top, :], raw[1, low, :]], axis=0), near, 0)
    pass_on((0, 0), 0)
    local[6].wait()
    absorb_queries(near, 0)

    total = later[...]
    for copy in pc:
        copy.wait_recv()
    for d in range(1, n_sp):
        total = total + later_in[d - 1]
    mods_later[tp] = total
    pd = []
    for i, peer in enumerate((far_tp, left_tp, right_tp)):
        copy = send(mods_later.at[tp], mods_later.at[tp], pd_send.at[i], pd_recv.at[i], {"tp": peer})
        copy.start()
        pd.append(copy)

    local[3].wait()
    x = key_value(modulated(context[...], 1))
    kv[n_sp, share : share + ctx_rows, :] = jnp.where(left, headed(x, kg), x).astype(jnp.bfloat16)

    def one(step, carry):
        group_sweep(step, first_half, slots(PAIRS, 0), FIRST_EVENTS)
        return carry

    lax.fori_loop(0, len(PAIRS), one, 0)

    far = [(left_tp, half, half), (right_tp, 0, half), (far_tp, 0, rows)]
    for i in range(2, 6):
        lat[i].wait_recv()
    absorb_keys(jnp.concatenate([raw[0, low, :], raw[1, top, :], raw[2]], axis=0), far, n_sp)
    pass_on((0, 0), 1)
    absorb_queries(far, n_half)

    def two(step, carry):
        group_sweep(step, second_half, slots(GROUPS, 0), EARLY_EVENTS)
        return carry

    lax.fori_loop(0, len(GROUPS), two, 0)

    def three(step, carry):
        group_sweep(step, second_half, slots(GROUPS, n_sp), LATE_EVENTS)
        return carry

    lax.fori_loop(0, len(GROUPS), three, 0)

    def done(b, o):
        o = (o[:HD] / o[HD : HD + 1]).astype(jnp.bfloat16).astype(jnp.float32)
        both = jnp.concatenate([o[:, :TILE], o[:, TILE:]], axis=0)
        pair, tile = b % n_half // tiles, b % n_half % tiles
        at = b // n_half * share + tile * TILE
        o_tok[at : at + TILE, pair * 2 * HD : (pair + 1) * 2 * HD] = both.T.astype(jnp.bfloat16)

    for slot in range(n_sp):
        kv_ctx[slot * ctx_rows : (slot + 1) * ctx_rows, :] = kv[n_sp + slot, share:, :]
    n_ctx = n_sp * ctx_rows
    span = group * HD
    mine = pl.ds(pl.multiple_of(tp * span, span), span)
    o_copies = []

    def finish(order):
        for b in order:
            done(b, acc[b])

    for t in range(n_ctx // TILE):
        v_t[:HD, t * TILE : (t + 1) * TILE] = kv_ctx[t * TILE : (t + 1) * TILE, :].T[HD:]
    units = [(b, lambda c: kv_ctx[c * KB : (c + 1) * KB, :], 0) for b in second_half + first_half]
    sweep(units, n_ctx, True, lambda b, o: done(b, o) if b >= n_half else acc.__setitem__(b, o))

    def send_back(at, count, owner, start):
        i = len(o_copies)
        copy = send(
            o_tok.at[at : at + count], o_all.at[start : start + count, mine],
            o_ssem.at[i], o_rsem.at[i], {"tp": owner},
        )
        copy.start()
        o_copies.append(copy)

    send_back(share + rows, rows, far_tp, 0)
    send_back(share, half, left_tp, half)
    send_back(share + half, half, right_tp, 0)

    wide = slots([GROUPS[0] + GROUPS[1], GROUPS[2] + GROUPS[3]], n_sp)
    mixed_blocks = [b for b in first_half if b % tiles > 0]
    own_blocks = [b for b in first_half if b % tiles == 0]

    def four(step, carry):
        group_sweep(step, mixed_blocks, wide, {})
        return carry

    lax.fori_loop(0, len(wide), four, 0)
    finish(mixed_blocks)
    send_back(rows, half, left_tp, 0)
    send_back(rows + half, half, right_tp, half)

    def five(step, carry):
        group_sweep(step, own_blocks, wide, {})
        return carry

    lax.fori_loop(0, len(wide), five, 0)
    finish(own_blocks)
    o_all[:, mine] = o_tok[0:rows, :]
    local[7].wait()

    def output(where):
        for j in range(n_tp):
            cols = pl.ds(j * chunk, chunk)
            y_j = jnp.dot(o_all[where, :], wout[:, cols], preferred_element_type=jnp.float32)
            gate = jnp.concatenate([mods_later[j, i : i + 1] for i in range(per_chunk)], axis=1)
            out[where, cols] = (latent[where, cols].astype(jnp.float32) + gate * y_j).astype(jnp.bfloat16)

    for copy in pd + o_copies:
        copy.wait_recv()
    output(slice(None))

    for copy in lat + pa + pb + pc + pd + o_copies:
        copy.wait_send()
    for index in range(len(flights)):
        flight(index, 0).wait_send()
        flight(index, 1).wait_send()


def on_device(n_sp, n_tp, latent, cond, cond_ctx, context, norm_gain, mod_shift, mod_scale, mod_gate,
              w_query, w_key, w_value, q_gain, k_gain, ctx_lift, w_out):
    _, rows, width = latent.shape
    tokens = rows * n_tp
    ctx_rows = context.shape[1]
    group = w_query.shape[1] // w_key.shape[1]
    keys = tokens + ctx_rows
    row_tab, col_tab = rope_tables(tokens * n_sp // GRID_W)
    chunk = mod_shift.shape[1]
    share = tokens // 2
    n_q = tokens // TILE * group // 2
    bf, f32 = jnp.bfloat16, jnp.float32
    vmem = pl.BlockSpec(memory_space=pltpu.VMEM)
    smem = pl.BlockSpec(memory_space=pltpu.SMEM)
    hbm = pl.BlockSpec(memory_space=pl.ANY)
    dma = pltpu.SemaphoreType.DMA
    out = pl.pallas_call(
        functools.partial(kernel, n_sp, n_tp, group),
        out_shape=jax.ShapeDtypeStruct((rows, width), bf),
        in_specs=[vmem] * 6 + [smem] + [vmem] * 2 + [hbm] * 8,
        out_specs=vmem,
        scratch_shapes=[
            pltpu.VMEM((ctx_rows, width), bf),
            pltpu.VMEM((3,) + mod_shift.shape, bf),
            pltpu.VMEM(w_query.shape, bf),
            pltpu.VMEM((2 * HD, width), bf),
            pltpu.VMEM(w_out.shape, bf),
            pltpu.VMEM((n_tp - 1, rows, width), bf),
            pltpu.VMEM((4 * chunk // TILE, TILE), f32),
            pltpu.VMEM((n_sp - 1, 4 * chunk // TILE, TILE), f32),
            pltpu.VMEM((2 * chunk // TILE, TILE), f32),
            pltpu.VMEM((n_sp - 1, 2 * chunk // TILE, TILE), f32),
            pltpu.VMEM((n_tp, 4 * chunk // TILE, TILE), f32),
            pltpu.VMEM((n_tp, 2 * chunk // TILE, TILE), f32),
            pltpu.VMEM((8, width), f32),
            pltpu.VMEM((2, tokens, 2 * HD), f32),
            pltpu.VMEM((share, width), bf),
            pltpu.VMEM((n_q, 4 * HD, QB), bf),
            pltpu.VMEM((2 * n_sp, share + ctx_rows, 2 * HD), bf),
            pltpu.VMEM((n_sp * ctx_rows, 2 * HD), bf),
            pltpu.VMEM((HD + 16, 4 * tokens), bf),
            pltpu.VMEM((AHEAD + 1, tokens, QB), f32),
            pltpu.VMEM((n_q, HD + 16, QB), f32),
            pltpu.VMEM((n_q, 8, QB), f32),
            pltpu.VMEM((tokens, group * HD), bf),
            pltpu.VMEM((rows, n_tp * group * HD), bf),
            dma((8,)),
            dma((6,)), dma((6,)),
            dma((n_sp - 1,)), dma((n_sp - 1,)),
            dma((n_tp - 1,)), dma((n_tp - 1,)),
            dma((n_sp - 1,)), dma((n_sp - 1,)),
            dma((n_tp - 1,)), dma((n_tp - 1,)),
            dma((2, n_sp - 1)), dma((2, n_sp)),
            dma((5,)), dma((5,)),
        ],
        compiler_params=pltpu.CompilerParams(
            collective_id=0, has_side_effects=True, vmem_limit_bytes=60 * 1024 * 1024,
        ),
    )(
        latent[0], cond, cond_ctx[None], norm_gain.reshape(width // TILE, TILE), q_gain[None], k_gain[None], ctx_lift,
        jnp.asarray(row_tab), jnp.asarray(col_tab),
        context[0], mod_shift, mod_scale, mod_gate, w_query, w_key.T, w_value.T, w_out,
    )
    return out[None]


def solution(mesh):
    placed = (
        P("dp", ("sp", "tp"), None),
        P("dp", "sp"),
        P("sp"),
        P("dp", "sp", None),
        P(),
        P("sp", "tp"),
        P("sp", "tp"),
        P("sp", "tp"),
        P(None, "tp"),
        P(None, "tp"),
        P(None, "tp"),
        P(),
        P(),
        P("tp"),
        P(),
    )
    return jax.shard_map(
        functools.partial(on_device, mesh.shape["sp"], mesh.shape["tp"]),
        mesh=mesh,
        in_specs=placed,
        out_specs=P("dp", ("sp", "tp"), None),
        check_vma=False,
    )
```
